128 devices in a mesh: ep: 64 (over z, y, x), tp: 2 (over core).
Axes of the slice: x: 4, y: 4, z: 4, core: 2. Of those that a mesh axis runs over, the one named last changes fastest.
Arguments:
- tokens: bfloat16 [1536, 4096], P('ep'), may hold values from -6 to 6
- cotangent: bfloat16 [1536, 4096], P('ep'), may hold values from -6 to 6
- routes: int32 [1536, 2], P('ep'), may hold values from 0 to 7, all different within a row; in each aligned block of 24 rows (0 to 23, 24 to 47, ...) at most 12 rows name the same one
- route_weights: float32 [1536, 2], P('ep'), may hold values from 0.1 to 0.9
- gate_weight: bfloat16 [64, 4096, 688], P('ep', None, 'tp'), may hold values from -0.09375 to 0.09375
- up_weight: bfloat16 [64, 4096, 688], P('ep', None, 'tp'), may hold values from -0.09375 to 0.09375
- down_weight: bfloat16 [64, 688, 4096], P('ep', 'tp'), may hold values from -0.078125 to 0.078125
Outputs:
- token_grad: bfloat16 [1536, 4096], P('ep', 'tp')
- route_grad: float32 [1536, 2], P('ep')
- gate_grad: bfloat16 [64, 4096, 688], P('ep', None, 'tp')
- up_grad: bfloat16 [64, 4096, 688], P('ep', None, 'tp')
- down_grad: bfloat16 [64, 688, 4096], P('ep', 'tp')
The draws below stay inside these ranges and needn't reach their ends.
Inputs may be any that keep to these rules, and one draw needn't show every extreme that they name: `routes`: each row names 2 different experts of 0 to 7; within the rows of one device (24 aligned rows) no expert is named more than 12 times, and in some blocks one is named exactly 12 times.
All inputs are finite; a program needn't handle non-finite values.
Results may differ from the reference program's by a relative error of at most 0.01.
Values may be sent and summed in bfloat16 or wider, within the bound.
No kernel may reach another device: no remote copies, remote signals or barrier semaphores. Data moves between devices by JAX's collectives and lax.ppermute only.
A program may use at most 192 MiB of HBM per device.

```python
import math
import jax
import jax.numpy as jnp
import numpy as np
from jax import lax

D = 4096
FF = 5504
EXPERTS = 8
TOP = 2
TOK_DEV = 24
CAP = 12
SPAN = 8
TOKENS = 1536
N_EP = 64


def shard_levels(stream_key, shape, split, least, top_value):
    def one(dim, shards_of):
        draws = jax.random.uniform(jax.random.fold_in(jax.random.fold_in(stream_key, 6), dim), (shards_of,), jnp.float32, least / len(split), top_value / len(split))
        return jnp.repeat(jnp.exp(draws), shape[dim] // shards_of).reshape((-1,) + (1,) * (len(shape) - dim - 1))

    gain = one(*split[0])
    for cut in split[1:]:
        gain = gain * one(*cut)
    return gain


def assign_block(rng, own, number, rows, count, top, most, slope):
    ranking = jax.random.permutation(rng, count)
    crowded, ordinary = load_shares(count, rows * top, most, slope, True), load_shares(count, rows * top, most, slope, False)
    places = jnp.arange(count)

    def named(lengths, offset_by):
        used = int((lengths > 0).sum())
        fixed = max(1, used // 4)
        moved = fixed + (places - fixed + offset_by * (used - fixed)) % max(1, count - fixed)
        return jnp.zeros((count,), jnp.int32).at[ranking[jnp.where(places < fixed, places, moved)]].set(jnp.asarray(lengths, jnp.int32))

    lengths = jnp.where(number % 4 == 0, named(crowded, number // 4), named(ordinary, number - number // 4 - 1))
    mixed = jax.random.permutation(jax.random.fold_in(own, 3), count)
    source_of, receiver = mixed[0:count // 2 * 2:2], mixed[1:count // 2 * 2:2]
    margin = jnp.minimum(lengths[source_of] - 1, most - lengths[receiver]) // 2
    margin = jnp.where((source_of == ranking[0]) | (receiver == ranking[0]) | (lengths[receiver] == 0), 0, jnp.maximum(margin, 0))
    moved = jax.random.randint(jax.random.fold_in(own, 4), (count // 2,), 0, 1 << 20) % (margin + 1)
    lengths = lengths.at[source_of].add(-moved).at[receiver].add(moved)
    items = jnp.searchsorted(jnp.cumsum(lengths), jnp.arange(rows * top), side="right").astype(jnp.int32)
    grid = items.reshape(top, rows).T
    grid = grid[jax.random.permutation(jax.random.fold_in(own, 1), rows)]
    offset_by = jax.random.randint(jax.random.fold_in(own, 2), (rows, 1), 0, top)
    return jnp.take_along_axis(grid, (jnp.arange(top)[None, :] + offset_by) % top, axis=1)


def load_shares(amount, total, reach, skew, full):
    loads = [(1 << 20) // math.isqrt(rank ** skew) + 1 for rank in range(1, amount + 1)]
    largest = reach if full else min(reach, max(-(-total // amount), total * loads[0] // sum(loads)))
    least = 1 if total - largest >= amount - 1 else 0
    given, surplus = [largest] + [least] * (amount - 1), total - largest - least * (amount - 1)
    while surplus > 0:
        free = [i for i in range(1, amount) if given[i] < largest] or [i for i in range(1, amount) if given[i] < reach]
        whole, left = sum([loads[i] for i in free]), surplus
        for i in free:
            addition = min(reach - given[i], max(1, left * loads[i] // whole), surplus)
            given[i] = given[i] + addition
            surplus = surplus - addition
    return np.array(given)


def bell_draw(stream_key, shape, spread, reach, pieces=(), kind=jnp.bfloat16):
    factor_of = shard_levels(stream_key, shape, pieces, -0.22, 0.18) if pieces else 1.0
    array = jax.random.normal(stream_key, shape, jnp.float32) * spread * factor_of
    return jnp.minimum(jnp.maximum(array, -reach), reach).astype(kind)


def setup_inputs(seed: int = 0) -> dict:
    splits = jax.random.split(jax.random.key(seed), 8)
    tokens = bell_draw(splits[0], (TOKENS, D), 1.0, 6.0, ((0, 64),))
    cotangent = bell_draw(splits[1], (TOKENS, D), 1.0, 6.0, ((0, 64),))
    routes_keys = jax.random.split(jax.random.fold_in(splits[2], 1), TOKENS // TOK_DEV)
    routes_turns = jax.random.permutation(jax.random.fold_in(splits[2], 3), TOKENS // TOK_DEV)
    routes = jax.vmap(lambda own, number: assign_block(jax.random.fold_in(splits[2], 2), own, number, TOK_DEV, EXPERTS, TOP, CAP, 2))(routes_keys, routes_turns).reshape((TOKENS, TOP))
    route_weights = jnp.clip(0.1 + 0.79999997 * jax.random.uniform(splits[3], (TOKENS, TOP), jnp.float32) ** shard_levels(splits[3], (TOKENS, TOP), ((0, 64),), -0.2, 0.2), 0.1, 0.9)
    gate_weight = bell_draw(splits[4], (EXPERTS * SPAN, D, FF // SPAN), D ** -0.5, 0.09375, ((0, 64), (2, 2)))
    up_weight = bell_draw(splits[5], (EXPERTS * SPAN, D, FF // SPAN), D ** -0.5, 0.09375, ((0, 64), (2, 2)))
    down_weight = bell_draw(splits[6], (EXPERTS * SPAN, FF // SPAN, D), FF ** -0.5, 0.078125, ((0, 64), (1, 2)))
    return {"tokens": tokens, "cotangent": cotangent, "routes": routes, "route_weights": route_weights, "gate_weight": gate_weight, "up_weight": up_weight, "down_weight": down_weight}


def silu_slope(pre_gate):
    sigma = jax.nn.sigmoid(pre_gate)
    return sigma * (1.0 + pre_gate * (1.0 - sigma))


def expert_pass(rows_in, rows_cot, shares, gate_mat, up_mat, down_mat):
    pre_gate = jnp.dot(rows_in, gate_mat, preferred_element_type=jnp.float32)
    pre_up = jnp.dot(rows_in, up_mat, preferred_element_type=jnp.float32)
    active = jax.nn.silu(pre_gate)
    hidden = (active * pre_up).astype(jnp.bfloat16)
    expert_out = jnp.dot(hidden, down_mat, preferred_element_type=jnp.float32)
    share_grad = jnp.sum(rows_cot.astype(jnp.float32) * expert_out, axis=1)
    scaled = (rows_cot.astype(jnp.float32) * shares[:, None]).astype(jnp.bfloat16)
    hidden_grad = lax.dot_general(scaled, down_mat, (((1,), (1,)), ((), ())), preferred_element_type=jnp.float32)
    gate_side = (hidden_grad * pre_up * silu_slope(pre_gate)).astype(jnp.bfloat16)
    up_side = (hidden_grad * active).astype(jnp.bfloat16)
    down_grad = lax.dot_general(hidden, scaled, (((0,), (0,)), ((), ())), preferred_element_type=jnp.float32).astype(jnp.bfloat16)
    gate_grad = lax.dot_general(rows_in, gate_side, (((0,), (0,)), ((), ())), preferred_element_type=jnp.float32).astype(jnp.bfloat16)
    up_grad = lax.dot_general(rows_in, up_side, (((0,), (0,)), ((), ())), preferred_element_type=jnp.float32).astype(jnp.bfloat16)
    token_part = lax.dot_general(gate_side, gate_mat, (((1,), (1,)), ((), ())), preferred_element_type=jnp.float32)
    token_part = token_part + lax.dot_general(up_side, up_mat, (((1,), (1,)), ((), ())), preferred_element_type=jnp.float32)
    return gate_grad, up_grad, down_grad, token_part, share_grad


def reference(tokens, cotangent, routes, route_weights, gate_weight, up_weight, down_weight):
    span = N_EP // EXPERTS
    block = FF // span
    listed = N_EP * CAP
    flat_routes = routes.reshape(-1)
    flat_shares = route_weights.reshape(-1)

    def one_expert(expert):
        chosen = flat_routes == expert
        count = jnp.sum(chosen.astype(jnp.int32))
        pairs = jnp.nonzero(chosen, size=listed, fill_value=0)[0].astype(jnp.int32)
        valid = jnp.arange(listed, dtype=jnp.int32) < count
        rows = (pairs // TOP).astype(jnp.int32)
        shares = jnp.where(valid, flat_shares[pairs], jnp.zeros_like(flat_shares[pairs]))
        start = (expert * span).astype(jnp.int32)
        gate_mat = lax.dynamic_slice_in_dim(gate_weight, start, span, 0).transpose(1, 0, 2).reshape(D, FF)
        up_mat = lax.dynamic_slice_in_dim(up_weight, start, span, 0).transpose(1, 0, 2).reshape(D, FF)
        down_mat = lax.dynamic_slice_in_dim(down_weight, start, span, 0).reshape(FF, D)
        gate_grad, up_grad, down_grad, token_part, share_grad = expert_pass(
            tokens[rows], cotangent[rows], shares, gate_mat, up_mat, down_mat)
        share_grad = jnp.where(valid, share_grad, jnp.zeros_like(share_grad))
        return (gate_grad.reshape(D, span, block).transpose(1, 0, 2),
                up_grad.reshape(D, span, block).transpose(1, 0, 2),
                down_grad.reshape(span, block, D), rows, pairs, token_part, share_grad)

    results = lax.map(one_expert, jnp.arange(EXPERTS, dtype=jnp.int32))
    gate_grad = results[0].reshape(EXPERTS * span, D, block)
    up_grad = results[1].reshape(EXPERTS * span, D, block)
    down_grad = results[2].reshape(EXPERTS * span, block, D)
    token_grad = jnp.zeros((TOKENS, D), jnp.float32).at[results[3].reshape(-1)].add(results[5].reshape(-1, D))
    route_grad = jnp.zeros((TOKENS * TOP,), jnp.float32).at[results[4].reshape(-1)].add(results[6].reshape(-1))
    return token_grad.astype(jnp.bfloat16), route_grad.reshape(TOKENS, TOP), gate_grad, up_grad, down_grad
```

```python
import jax
import jax.numpy as jnp
from jax import lax
from jax.sharding import Mesh
from jax.sharding import PartitionSpec as P

EXPERTS = 8
TOP = 2
CAP = 12
ROOM = 16
BF = jnp.bfloat16
F32 = jnp.float32


def along_x(value, step):
    return lax.ppermute(value, "x", [(i, (i + step) % 4) for i in range(4)])


def pair_y(value):
    return lax.ppermute(value, "yl", [(0, 1), (1, 0)])


def pair_core(value):
    return lax.ppermute(value, "core", [(0, 1), (1, 0)])


def to_expert(value, dz, dy, sign):
    perm = []
    for z in range(4):
        for y in range(4):
            there = (z + sign * dz) % 4 * 4 + (3 - y if dy else y)
            perm.append((z * 4 + y, there))
    return lax.ppermute(value, ("z", "yh", "yl"), perm)


def dot_f32(a, b, dims):
    return lax.dot_general(a, b, (dims, ((), ())), preferred_element_type=F32)


def per_device(tokens, cotangent, routes, route_weights, gate_weight, up_weight, down_weight):
    z = lax.axis_index("z")
    yh = lax.axis_index("yh")
    core = lax.axis_index("core")
    rows, width = tokens.shape
    half = width // 2
    hid = gate_weight.shape[2]
    lanes = -(-hid // 128) * 128
    first = core == 0

    def mine(w, axis):
        return lax.dynamic_slice_in_dim(w, core * half, half, axis)

    def others(w, axis):
        return lax.dynamic_slice_in_dim(w, (1 - core) * half, half, axis)

    def both(w, axis):
        own = mine(w, axis)
        got = pair_core(others(w, axis))
        pads = [(0, 0), (0, 0)]
        pads[1 - axis] = (0, lanes - hid)
        a = jnp.pad(jnp.where(first, own, got), pads)
        b = jnp.pad(jnp.where(first, got, own), pads)
        return jnp.concatenate([a, b], axis=1 - axis)

    order = jnp.arange(EXPERTS, dtype=jnp.int32)
    expert_of = 2 * ((z + order // 2) % 4) + (yh + order % 2) % 2
    flat_routes = routes.reshape(-1)
    pairs = rows * TOP
    hot = flat_routes[None, :] == expert_of[:, None]
    tri = jnp.arange(pairs)[:, None] < jnp.arange(pairs)[None, :]
    position = jnp.dot(hot.astype(BF), tri.astype(BF), preferred_element_type=F32)
    room = jnp.arange(ROOM, dtype=jnp.int32).astype(F32)
    placing = (hot[:, None, :] & (position[:, None, :] == room[None, :, None])).reshape(
        EXPERTS * ROOM, pairs
    )
    place = placing.astype(BF)
    flat_weights = route_weights.reshape(-1)
    token_half = lax.dynamic_slice_in_dim(tokens, core * half, half, 1)
    cot_half = lax.dynamic_slice_in_dim(cotangent, core * half, half, 1)
    slot_weight = jnp.sum(jnp.where(placing, flat_weights[None, :], 0.0), axis=1)
    place_token = jnp.sum(place.reshape(EXPERTS * ROOM, rows, TOP), axis=2)
    slot_tokens = dot_f32(place_token, token_half, ((1,), (0,))).astype(BF)
    slot_cot = dot_f32(place_token, cot_half, ((1,), (0,)))
    slot_scaled = (slot_cot * slot_weight[:, None]).astype(BF)
    send = jnp.concatenate([slot_tokens, slot_scaled], axis=1)
    offsets = [(dz, dy) for dz in range(4) for dy in range(2)]
    pieces = [
        send[:ROOM] if k == 0 else to_expert(send[ROOM * k : ROOM * (k + 1)], *o, 1)
        for k, o in enumerate(offsets)
    ]
    packed = EXPERTS * CAP
    row_of = jnp.arange(packed)
    pack = (
        (row_of // CAP * ROOM + row_of % CAP)[:, None] == jnp.arange(EXPERTS * ROOM)[None, :]
    ).astype(BF)
    own = dot_f32(pack, jnp.concatenate(pieces, axis=0), ((1,), (0,))).astype(BF)

    left = along_x(own, 1)
    right = along_x(own, -1)
    partner = pair_y(own)
    far_left = along_x(partner, 1)
    far_right = pair_y(right)
    across = along_x(right, -1)
    third = packed // 3
    last = [
        along_x(far_left[:third], 1),
        along_x(far_right[third : 2 * third], -1),
        pair_y(across[2 * third :]),
    ]

    gate_both = both(gate_weight[0], 0)
    up_both = both(up_weight[0], 0)
    gate_up = jnp.concatenate([gate_both, up_both], axis=1)
    down_both = both(down_weight[0], 1)
    full = 2 * lanes

    def forward(parts):
        block = jnp.concatenate(parts, axis=0)
        ins, scaled = block[:, :half], block[:, half:]
        pre = dot_f32(ins, gate_up, ((1,), (0,))).astype(BF)
        grad = dot_f32(scaled, down_both, ((1,), (1,))).astype(BF)
        return ins, scaled, jnp.concatenate([pre, grad], axis=1)

    def sides(partial, received):
        total = partial.astype(F32) + received.astype(F32)
        gate, up, grad = total[:, :full], total[:, full : 2 * full], total[:, 2 * full :]
        sigma = jax.nn.sigmoid(gate)
        active = gate * sigma
        hidden = (active * up).astype(BF)
        gate_side = (grad * up * (sigma * (1.0 + gate * (1.0 - sigma)))).astype(BF)
        up_side = (grad * active).astype(BF)
        share = jnp.sum(hidden.astype(F32) * grad, axis=1, keepdims=True)
        return jnp.concatenate([gate_side, up_side], axis=1), hidden, share

    groups = [[own, left, right, partner], [far_left, far_right, across], last]
    kept = []
    terms = []
    for parts in groups:
        ins, scaled, partial = forward(parts)
        side, hidden, share = sides(partial, pair_core(partial))
        token_term = dot_f32(side, gate_up, ((1,), (1,))).astype(BF)
        share_term = jnp.pad(share.astype(BF), ((0, 0), (0, 127)))
        terms.append(jnp.concatenate([token_term, share_term], axis=1))
        kept.append((ins, scaled, side, hidden))

    def chunk(g, i):
        return terms[g][packed * i : packed * (i + 1)]

    def add(a, *more):
        total = a.astype(F32)
        for m in more:
            total = total + m.astype(F32)
        return total.astype(BF)

    t_last = terms[2]
    a_left = along_x(t_last[:third], -1)
    a_right = along_x(t_last[third : 2 * third], 1)
    a_pair = pair_y(t_last[2 * third :])
    t_far_left = jnp.concatenate(
        [add(chunk(1, 0)[:third], a_left), chunk(1, 0)[third:]], axis=0
    )
    t_far_right = jnp.concatenate(
        [
            chunk(1, 1)[:third],
            add(chunk(1, 1)[third : 2 * third], a_right),
            chunk(1, 1)[2 * third :],
        ],
        axis=0,
    )
    t_across = jnp.concatenate(
        [chunk(1, 2)[: 2 * third], add(chunk(1, 2)[2 * third :], a_pair)], axis=0
    )
    b_partner = along_x(t_far_left, -1)
    b_right_pair = pair_y(t_far_right)
    b_right = along_x(t_across, 1)
    c_left = along_x(chunk(0, 1), -1)
    c_right = along_x(add(chunk(0, 2), b_right_pair, b_right), 1)
    c_pair = pair_y(add(chunk(0, 3), b_partner))
    home = add(chunk(0, 0), c_left, c_right, c_pair)

    spread = dot_f32(pack, home, ((0,), (0,))).astype(BF)
    back = jnp.concatenate(
        [
            spread[:ROOM] if k == 0 else to_expert(spread[ROOM * k : ROOM * (k + 1)], *o, -1)
            for k, o in enumerate(offsets)
        ],
        axis=0,
    )
    token_grad = dot_f32(place_token, back[:, :half], ((0,), (0,))).astype(BF)
    slot_share = back[:, half : half + 1].astype(F32)
    pair_share = jnp.sum(jnp.where(placing, slot_share, 0.0), axis=0)
    route_grad = (pair_share / flat_weights).reshape(rows, TOP)

    all_ins = jnp.concatenate([k[0] for k in kept], axis=0)
    all_scaled = jnp.concatenate([k[1] for k in kept], axis=0)
    all_side = jnp.concatenate([k[2] for k in kept], axis=0)
    all_hidden = jnp.concatenate([k[3] for k in kept], axis=0)

    def joined(grad, axis):
        own_part = lax.dynamic_slice_in_dim(grad, core * lanes, lanes, 1 - axis)
        other_part = lax.dynamic_slice_in_dim(grad, (1 - core) * lanes, lanes, 1 - axis)
        own_part = lax.slice_in_dim(own_part, 0, hid, axis=1 - axis)
        other_part = lax.slice_in_dim(other_part, 0, hid, axis=1 - axis)
        got = pair_core(other_part)
        return jnp.concatenate(
            [jnp.where(first, own_part, got), jnp.where(first, got, own_part)], axis=axis
        )

    side_grad = dot_f32(all_ins, all_side, ((0,), (0,))).astype(BF)
    gate_grad = joined(side_grad[:, :full], 0)
    up_grad = joined(side_grad[:, full:], 0)
    down_grad = joined(dot_f32(all_hidden, all_scaled, ((0,), (0,))).astype(BF), 1)
    return token_grad, route_grad, gate_grad[None], up_grad[None], down_grad[None]


def solution(mesh):
    names = ("z", "yh", "yl", "x", "core")
    fine = Mesh(mesh.devices.reshape(4, 2, 2, 4, 2), names)
    ep = names[:4]
    return jax.shard_map(
        per_device,
        mesh=fine,
        in_specs=(
            P(ep, None),
            P(ep, None),
            P(ep, None),
            P(ep, None),
            P(ep, None, "core"),
            P(ep, None, "core"),
            P(ep, "core", None),
        ),
        out_specs=(
            P(ep, "core"),
            P(ep, None),
            P(ep, None, "core"),
            P(ep, None, "core"),
            P(ep, "core", None),
        ),
        check_vma=False,
    )
```

```python
import functools

import jax
import jax.numpy as jnp
from jax import lax
from jax.experimental import pallas as pl
from jax.experimental.pallas import tpu as pltpu
from jax.sharding import Mesh
from jax.sharding import PartitionSpec as P

EXPERTS = 8
TOP = 2
CAP = 12
ROOM = 16
LANES = 128
BF = jnp.bfloat16
F32 = jnp.float32
MIB = 1 << 20


VMEM = pl.BlockSpec(memory_space=pltpu.VMEM)
SMEM = pl.BlockSpec(memory_space=pltpu.SMEM)


def along_x(value, step):
    return lax.ppermute(value, "x", [(i, (i + step) % 4) for i in range(4)])


def pair_y(value):
    return lax.ppermute(value, "yl", [(0, 1), (1, 0)])


def pair_core(value):
    return lax.ppermute(value, "core", [(0, 1), (1, 0)])


def to_expert(value, dz, dy, sign):
    perm = []
    for z in range(4):
        for y in range(4):
            there = (z + sign * dz) % 4 * 4 + (3 - y if dy else y)
            perm.append((z * 4 + y, there))
    return lax.ppermute(value, ("z", "yh", "yl"), perm)


def dot_f32(a, b, left, right):
    return lax.dot_general(a, b, (((left,), (right,)), ((), ())), preferred_element_type=F32)


def slots_kernel(half, place_ref, tok_ref, cot_ref, routes_ref, weights_ref, *outs):
    core, z, yh = place_ref[0], place_ref[1], place_ref[2]
    first_ref, second_ref = outs[EXPERTS:]
    rows = tok_ref.shape[0]
    slot = lax.broadcasted_iota(jnp.int32, (rows, EXPERTS * ROOM), 1)
    index = slot // ROOM
    expert = 2 * ((z + index // 2) % 4) + (yh + index % 2) % 2
    is_first = routes_ref[:, 0:1] == expert
    is_second = routes_ref[:, 1:2] == expert
    hot = jnp.where(is_first | is_second, 1.0, 0.0).astype(BF)
    below = lax.broadcasted_iota(jnp.int32, (rows, rows), 1) < lax.broadcasted_iota(
        jnp.int32, (rows, rows), 0
    )
    position = dot_f32(jnp.where(below, 1.0, 0.0).astype(BF), hot, 1, 0)
    fits = position == (slot % ROOM).astype(F32)
    first = jnp.where(is_first & fits, 1.0, 0.0).astype(BF)
    second = jnp.where(is_second & fits, 1.0, 0.0).astype(BF)
    first_ref[...] = first
    second_ref[...] = second
    here = pl.ds(pl.multiple_of(core * half, half), half)
    slot_tok = dot_f32(first + second, tok_ref[:, here], 0, 0).astype(BF)
    cot = cot_ref[:, here].astype(F32)
    scaled = dot_f32(first, (cot * weights_ref[:, 0:1]).astype(BF), 0, 0)
    scaled = scaled + dot_f32(second, (cot * weights_ref[:, 1:2]).astype(BF), 0, 0)
    scaled = scaled.astype(BF)
    for k in range(EXPERTS):
        outs[k][:, :half] = slot_tok[k * ROOM : (k + 1) * ROOM]
        outs[k][:, half:] = scaled[k * ROOM : (k + 1) * ROOM]


def make_slots(place, tokens, cotangent, routes, weights):
    rows, width = tokens.shape
    shapes = [jax.ShapeDtypeStruct((ROOM, width), BF)] * EXPERTS
    shapes += [jax.ShapeDtypeStruct((rows, EXPERTS * ROOM), BF)] * 2
    return pl.pallas_call(
        functools.partial(slots_kernel, width // 2),
        out_shape=shapes,
        in_specs=[SMEM] + [VMEM] * 4,
        out_specs=[VMEM] * len(shapes),
        compiler_params=pltpu.CompilerParams(vmem_limit_bytes=8 * MIB),
        cost_estimate=pl.CostEstimate(
            flops=2 * 128 * 24 * width * 2, bytes_accessed=3 * MIB, transcendentals=0
        ),
        name="slots",
    )(place, tokens, cotangent, routes, weights)


def group_kernel(count, half, place_ref, *refs):
    core = place_ref[0]
    ours, theirs = refs[:count], refs[count : 2 * count]
    gate_ref, up_ref, down_ref = refs[2 * count : 2 * count + 3]
    keep_ref, send_ref, gate_out, up_out, hidden_out = refs[2 * count + 3 :]
    here = pl.ds(pl.multiple_of(core * half, half), half)
    there = pl.ds(pl.multiple_of((1 - core) * half, half), half)
    tok = [jnp.concatenate([r[:, :half] for r in side], axis=0) for side in (ours, theirs)]
    gate = dot_f32(tok[0], gate_ref[:, here], 1, 1) + dot_f32(tok[1], gate_ref[:, there], 1, 1)
    up = dot_f32(tok[0], up_ref[:, here], 1, 1) + dot_f32(tok[1], up_ref[:, there], 1, 1)
    cot = [jnp.concatenate([r[:, half:] for r in side], axis=0) for side in (ours, theirs)]
    grad = dot_f32(cot[0], down_ref[:, here], 1, 1) + dot_f32(cot[1], down_ref[:, there], 1, 1)
    sigma = 1.0 / (1.0 + jnp.exp(-gate))
    active = gate * sigma
    hidden = (active * up).astype(BF)
    gate_side = (grad * up * (sigma * (1.0 + gate * (1.0 - sigma)))).astype(BF)
    up_side = (grad * active).astype(BF)
    hidden_out[...] = hidden
    gate_out[...] = gate_side
    up_out[...] = up_side
    share = jnp.sum(hidden.astype(F32) * grad, axis=1, keepdims=True).astype(BF)
    share = jnp.broadcast_to(share, (share.shape[0], LANES))
    for where, out in ((here, keep_ref), (there, send_ref)):
        term = dot_f32(gate_side, gate_ref[:, where], 1, 0)
        term = term + dot_f32(up_side, up_ref[:, where], 1, 0)
        out[:, :half] = term.astype(BF)
        out[:, half:] = share


def run_group(place, ours, theirs, gate, up, down):
    rows = sum(r.shape[0] for r in ours)
    hid, width = gate.shape
    half = width // 2
    shapes = [jax.ShapeDtypeStruct((rows, half + LANES), BF)] * 2
    shapes += [jax.ShapeDtypeStruct((rows, hid), BF)] * 3
    return pl.pallas_call(
        functools.partial(group_kernel, len(ours), half),
        out_shape=shapes,
        in_specs=[SMEM] + [VMEM] * (2 * len(ours) + 3),
        out_specs=[VMEM] * len(shapes),
        compiler_params=pltpu.CompilerParams(vmem_limit_bytes=40 * MIB),
        cost_estimate=pl.CostEstimate(
            flops=10 * rows * hid * width, bytes_accessed=16 * MIB, transcendentals=rows * hid
        ),
        name="group",
    )(place, *ours, *theirs, gate, up, down)


def weight_kernel(count, half, offset, sides, place_ref, *refs):
    core = place_ref[0]
    ours, theirs = refs[:count], refs[count : 2 * count]
    side_refs = refs[2 * count : 2 * count + 2 * sides]
    outs = refs[2 * count + 2 * sides :]
    here = pl.ds(pl.multiple_of(core * half, half), half)
    there = pl.ds(pl.multiple_of((1 - core) * half, half), half)
    for group, where in ((ours, here), (theirs, there)):
        block = jnp.concatenate([r[:, offset : offset + half] for r in group], axis=0)
        for i in range(sides):
            side = jnp.concatenate([side_refs[2 * i][...], side_refs[2 * i + 1][...]], axis=0)
            outs[i][:, where] = dot_f32(side, block, 0, 0).astype(BF)


def weight_grads(place, ours, theirs, side_pairs, offset):
    rows = sum(r.shape[0] for r in ours)
    hid = side_pairs[0][0].shape[1]
    width = ours[0].shape[1]
    shapes = [jax.ShapeDtypeStruct((hid, width), BF)] * len(side_pairs)
    flat = [s for pair in side_pairs for s in pair]
    return pl.pallas_call(
        functools.partial(weight_kernel, len(ours), width // 2, offset, len(side_pairs)),
        out_shape=shapes,
        in_specs=[SMEM] + [VMEM] * (2 * len(ours) + len(flat)),
        out_specs=[VMEM] * len(shapes),
        compiler_params=pltpu.CompilerParams(vmem_limit_bytes=52 * MIB),
        cost_estimate=pl.CostEstimate(
            flops=2 * rows * hid * width * len(side_pairs),
            bytes_accessed=16 * MIB,
            transcendentals=0,
        ),
        name="weight_grads",
    )(place, *ours, *theirs, *flat)


def final_kernel(half, weights_ref, first_ref, second_ref, *refs):
    backs = refs[:EXPERTS]
    token_ref, route_ref = refs[EXPERTS:]
    back = jnp.concatenate([b[...] for b in backs], axis=0)
    first, second = first_ref[...], second_ref[...]
    token_ref[...] = dot_f32(first + second, back[:, :half], 1, 0).astype(BF)
    share = back[:, half:]
    route_ref[:, 0:1] = dot_f32(first, share, 1, 0)[:, 0:1] / weights_ref[:, 0:1]
    route_ref[:, 1:2] = dot_f32(second, share, 1, 0)[:, 0:1] / weights_ref[:, 1:2]


def combine(weights, first, second, backs):
    rows = weights.shape[0]
    half = backs[0].shape[1] - LANES
    return pl.pallas_call(
        functools.partial(final_kernel, half),
        out_shape=[
            jax.ShapeDtypeStruct((rows, half), BF),
            jax.ShapeDtypeStruct((rows, TOP), F32),
        ],
        in_specs=[VMEM] * (3 + EXPERTS),
        out_specs=[VMEM] * 2,
        compiler_params=pltpu.CompilerParams(vmem_limit_bytes=8 * MIB),
        cost_estimate=pl.CostEstimate(
            flops=2 * 128 * 24 * half, bytes_accessed=MIB, transcendentals=0
        ),
        name="combine",
    )(weights, first, second, *backs)


def per_device(tokens, cotangent, routes, route_weights, gate_weight, up_weight, down_weight):
    place = jnp.stack([lax.axis_index("core"), lax.axis_index("z"), lax.axis_index("yh")])
    place = place.astype(jnp.int32)
    offsets = [(dz, dy) for dz in range(4) for dy in range(2)]
    packed = EXPERTS * CAP
    third = packed // 3

    made = make_slots(place, tokens, cotangent, routes, route_weights)
    first, second = made[EXPERTS:]
    pieces = [made[0]] + [to_expert(made[k], *offsets[k], 1) for k in range(1, EXPERTS)]
    row_of = jnp.arange(packed)
    pack = (
        (row_of // CAP * ROOM + row_of % CAP)[:, None] == jnp.arange(EXPERTS * ROOM)[None, :]
    ).astype(BF)
    own = dot_f32(pack, jnp.concatenate(pieces, axis=0), 1, 0).astype(BF)

    left = along_x(own, 1)
    right = along_x(own, -1)
    partner = pair_y(own)
    far_left = along_x(partner, 1)
    far_right = pair_y(right)
    across = along_x(right, -1)
    last = [
        along_x(far_left[:third], 1),
        along_x(far_right[third : 2 * third], -1),
        pair_y(across[2 * third :]),
    ]

    gate_t = gate_weight[0].T
    up_t = up_weight[0].T
    down_t = down_weight[0]
    near = [own, left, right, partner]
    far = [far_left, far_right, across] + last
    near_other = [pair_core(v) for v in near]
    far_other = [pair_core(v) for v in far]
    near_out = run_group(place, near, near_other, gate_t, up_t, down_t)
    far_out = run_group(place, far, far_other, gate_t, up_t, down_t)

    def add(a, *more):
        total = a.astype(F32)
        for m in more:
            total = total + m.astype(F32)
        return total.astype(BF)

    near_got = pair_core(near_out[1])
    far_got = pair_core(far_out[1])

    def chunk(out, got, i, a=0, b=packed):
        return add(out[0][packed * i + a : packed * i + b], got[packed * i + a : packed * i + b])

    t_last = [chunk(far_out, far_got, 3, third * i, third * (i + 1)) for i in range(3)]
    a_left = along_x(t_last[0], -1)
    a_right = along_x(t_last[1], 1)
    a_pair = pair_y(t_last[2])
    pads = [[(third * i, packed - third * (i + 1)), (0, 0)] for i in range(3)]
    t_far_left = add(chunk(far_out, far_got, 0), jnp.pad(a_left, pads[0]))
    t_far_right = add(chunk(far_out, far_got, 1), jnp.pad(a_right, pads[1]))
    t_across = add(chunk(far_out, far_got, 2), jnp.pad(a_pair, pads[2]))
    b_partner = along_x(t_far_left, -1)
    b_right_pair = pair_y(t_far_right)
    b_right = along_x(t_across, 1)
    c_left = along_x(chunk(near_out, near_got, 1), -1)
    c_right = along_x(add(chunk(near_out, near_got, 2), b_right_pair, b_right), 1)
    c_pair = pair_y(add(chunk(near_out, near_got, 3), b_partner))
    home = add(chunk(near_out, near_got, 0), c_left, c_right, c_pair)

    spread = dot_f32(pack, home, 0, 0).astype(BF)
    backs = [spread[:ROOM]] + [
        to_expert(spread[ROOM * k : ROOM * (k + 1)], *offsets[k], -1) for k in range(1, EXPERTS)
    ]
    token_grad, route_grad = combine(route_weights, first, second, backs)

    ours, theirs = near + far, near_other + far_other
    half = tokens.shape[1] // 2
    gate_grad, up_grad = weight_grads(
        place, ours, theirs, [(near_out[2], far_out[2]), (near_out[3], far_out[3])], 0
    )
    (down_grad,) = weight_grads(place, ours, theirs, [(near_out[4], far_out[4])], half)
    return token_grad, route_grad, gate_grad.T[None], up_grad.T[None], down_grad[None]


def solution(mesh):
    names = ("z", "yh", "yl", "x", "core")
    fine = Mesh(mesh.devices.reshape(4, 2, 2, 4, 2), names)
    ep = names[:4]
    return jax.shard_map(
        per_device,
        mesh=fine,
        in_specs=(
            P(ep, None),
            P(ep, None),
            P(ep, None),
            P(ep, None),
            P(ep, None, "core"),
            P(ep, None, "core"),
            P(ep, "core", None),
        ),
        out_specs=(
            P(ep, "core"),
            P(ep, None),
            P(ep, None, "core"),
            P(ep, None, "core"),
            P(ep, "core", None),
        ),
        check_vma=False,
    )
```

```python
import functools

import jax
import jax.numpy as jnp
from jax import lax
from jax.experimental import pallas as pl
from jax.experimental.pallas import tpu as pltpu
from jax.sharding import Mesh
from jax.sharding import PartitionSpec as P

EXPERTS = 8
TOP = 2
CAP = 12
ROOM = 16
LANES = 128
BF = jnp.bfloat16
F32 = jnp.float32
MIB = 1 << 20


VMEM = pl.BlockSpec(memory_space=pltpu.VMEM)
SMEM = pl.BlockSpec(memory_space=pltpu.SMEM)


def along_x(value, step):
    return lax.ppermute(value, "x", [(i, (i + step) % 4) for i in range(4)])


def pair_y(value):
    return lax.ppermute(value, "yl", [(0, 1), (1, 0)])


def pair_core(value):
    return lax.ppermute(value, "core", [(0, 1), (1, 0)])


def to_expert(value, dz, dy, sign):
    perm = []
    for z in range(4):
        for y in range(4):
            there = (z + sign * dz) % 4 * 4 + (3 - y if dy else y)
            perm.append((z * 4 + y, there))
    return lax.ppermute(value, ("z", "yh", "yl"), perm)


def dot_f32(a, b, left, right):
    return lax.dot_general(a, b, (((left,), (right,)), ((), ())), preferred_element_type=F32)


def slots_kernel(half, place_ref, tok_ref, cot_ref, routes_ref, weights_ref, *outs):
    core, z, yh = place_ref[0], place_ref[1], place_ref[2]
    first_ref, second_ref = outs[EXPERTS:]
    rows = tok_ref.shape[0]
    slot = lax.broadcasted_iota(jnp.int32, (rows, EXPERTS * ROOM), 1)
    index = slot // ROOM
    expert = 2 * ((z + index // 2) % 4) + (yh + index % 2) % 2
    is_first = routes_ref[:, 0:1] == expert
    is_second = routes_ref[:, 1:2] == expert
    hot = jnp.where(is_first | is_second, 1.0, 0.0).astype(BF)
    below = lax.broadcasted_iota(jnp.int32, (rows, rows), 1) < lax.broadcasted_iota(
        jnp.int32, (rows, rows), 0
    )
    position = dot_f32(jnp.where(below, 1.0, 0.0).astype(BF), hot, 1, 0)
    fits = position == (slot % ROOM).astype(F32)
    first = jnp.where(is_first & fits, 1.0, 0.0).astype(BF)
    second = jnp.where(is_second & fits, 1.0, 0.0).astype(BF)
    first_ref[...] = first
    second_ref[...] = second
    here = pl.ds(pl.multiple_of(core * half, half), half)
    slot_tok = dot_f32(first + second, tok_ref[:, here], 0, 0).astype(BF)
    cot = cot_ref[:, here].astype(F32)
    scaled = dot_f32(first, (cot * weights_ref[:, 0:1]).astype(BF), 0, 0)
    scaled = scaled + dot_f32(second, (cot * weights_ref[:, 1:2]).astype(BF), 0, 0)
    scaled = scaled.astype(BF)
    for k in range(EXPERTS):
        outs[k][:, :half] = slot_tok[k * ROOM : (k + 1) * ROOM]
        outs[k][:, half:] = scaled[k * ROOM : (k + 1) * ROOM]


def make_slots(place, tokens, cotangent, routes, weights):
    rows, width = tokens.shape
    shapes = [jax.ShapeDtypeStruct((ROOM, width), BF)] * EXPERTS
    shapes += [jax.ShapeDtypeStruct((rows, EXPERTS * ROOM), BF)] * 2
    return pl.pallas_call(
        functools.partial(slots_kernel, width // 2),
        out_shape=shapes,
        in_specs=[SMEM] + [VMEM] * 4,
        out_specs=[VMEM] * len(shapes),
        compiler_params=pltpu.CompilerParams(vmem_limit_bytes=8 * MIB),
        cost_estimate=pl.CostEstimate(
            flops=2 * 128 * 24 * width * 2, bytes_accessed=3 * MIB, transcendentals=0
        ),
        name="slots",
    )(place, tokens, cotangent, routes, weights)


def group_kernel(count, half, place_ref, *refs):
    core = place_ref[0]
    ours, theirs = refs[:count], refs[count : 2 * count]
    gate_ref, up_ref, down_ref = refs[2 * count : 2 * count + 3]
    keep_ref, send_ref, gate_out, up_out, hidden_out = refs[2 * count + 3 :]
    here = pl.ds(pl.multiple_of(core * half, half), half)
    there = pl.ds(pl.multiple_of((1 - core) * half, half), half)
    tok = [jnp.concatenate([r[:, :half] for r in side], axis=0) for side in (ours, theirs)]
    gate = dot_f32(tok[0], gate_ref[:, here], 1, 1) + dot_f32(tok[1], gate_ref[:, there], 1, 1)
    up = dot_f32(tok[0], up_ref[:, here], 1, 1) + dot_f32(tok[1], up_ref[:, there], 1, 1)
    cot = [jnp.concatenate([r[:, half:] for r in side], axis=0) for side in (ours, theirs)]
    grad = dot_f32(cot[0], down_ref[:, here], 1, 1) + dot_f32(cot[1], down_ref[:, there], 1, 1)
    sigma = 1.0 / (1.0 + jnp.exp(-gate))
    active = gate * sigma
    hidden = (active * up).astype(BF)
    gate_side = (grad * up * (sigma * (1.0 + gate * (1.0 - sigma)))).astype(BF)
    up_side = (grad * active).astype(BF)
    hidden_out[...] = hidden
    gate_out[...] = gate_side
    up_out[...] = up_side
    share = jnp.sum(hidden.astype(F32) * grad, axis=1, keepdims=True).astype(BF)
    share = jnp.broadcast_to(share, (share.shape[0], LANES))
    for where, out in ((here, keep_ref), (there, send_ref)):
        term = dot_f32(gate_side, gate_ref[:, where], 1, 0)
        term = term + dot_f32(up_side, up_ref[:, where], 1, 0)
        out[:, :half] = term.astype(BF)
        out[:, half:] = share


def run_group(place, ours, theirs, gate, up, down):
    rows = sum(r.shape[0] for r in ours)
    hid, width = gate.shape
    half = width // 2
    shapes = [jax.ShapeDtypeStruct((rows, half + LANES), BF)] * 2
    shapes += [jax.ShapeDtypeStruct((rows, hid), BF)] * 3
    return pl.pallas_call(
        functools.partial(group_kernel, len(ours), half),
        out_shape=shapes,
        in_specs=[SMEM] + [VMEM] * (2 * len(ours) + 3),
        out_specs=[VMEM] * len(shapes),
        compiler_params=pltpu.CompilerParams(vmem_limit_bytes=40 * MIB),
        cost_estimate=pl.CostEstimate(
            flops=10 * rows * hid * width, bytes_accessed=16 * MIB, transcendentals=rows * hid
        ),
        name="group",
    )(place, *ours, *theirs, gate, up, down)


def weight_kernel(count, half, offset, sides, place_ref, *refs):
    core = place_ref[0]
    ours, theirs = refs[:count], refs[count : 2 * count]
    side_refs = refs[2 * count : 2 * count + 2 * sides]
    outs = refs[2 * count + 2 * sides :]
    here = pl.ds(pl.multiple_of(core * half, half), half)
    there = pl.ds(pl.multiple_of((1 - core) * half, half), half)
    for group, where in ((ours, here), (theirs, there)):
        block = jnp.concatenate([r[:, offset : offset + half] for r in group], axis=0)
        for i in range(sides):
            side = jnp.concatenate([side_refs[2 * i][...], side_refs[2 * i + 1][...]], axis=0)
            outs[i][:, where] = dot_f32(side, block, 0, 0).astype(BF)


def weight_grads(place, ours, theirs, side_pairs, offset):
    rows = sum(r.shape[0] for r in ours)
    hid = side_pairs[0][0].shape[1]
    width = ours[0].shape[1]
    shapes = [jax.ShapeDtypeStruct((hid, width), BF)] * len(side_pairs)
    flat = [s for pair in side_pairs for s in pair]
    return pl.pallas_call(
        functools.partial(weight_kernel, len(ours), width // 2, offset, len(side_pairs)),
        out_shape=shapes,
        in_specs=[SMEM] + [VMEM] * (2 * len(ours) + len(flat)),
        out_specs=[VMEM] * len(shapes),
        compiler_params=pltpu.CompilerParams(vmem_limit_bytes=52 * MIB),
        cost_estimate=pl.CostEstimate(
            flops=2 * rows * hid * width * len(side_pairs),
            bytes_accessed=16 * MIB,
            transcendentals=0,
        ),
        name="weight_grads",
    )(place, *ours, *theirs, *flat)


def final_kernel(half, weights_ref, first_ref, second_ref, *refs):
    backs = refs[:EXPERTS]
    token_ref, route_ref = refs[EXPERTS:]
    back = jnp.concatenate([b[...] for b in backs], axis=0)
    first, second = first_ref[...], second_ref[...]
    token_ref[...] = dot_f32(first + second, back[:, :half], 1, 0).astype(BF)
    share = back[:, half:]
    route_ref[:, 0:1] = dot_f32(first, share, 1, 0)[:, 0:1] / weights_ref[:, 0:1]
    route_ref[:, 1:2] = dot_f32(second, share, 1, 0)[:, 0:1] / weights_ref[:, 1:2]


def combine(weights, first, second, backs):
    rows = weights.shape[0]
    half = backs[0].shape[1] - LANES
    return pl.pallas_call(
        functools.partial(final_kernel, half),
        out_shape=[
            jax.ShapeDtypeStruct((rows, half), BF),
            jax.ShapeDtypeStruct((rows, TOP), F32),
        ],
        in_specs=[VMEM] * (3 + EXPERTS),
        out_specs=[VMEM] * 2,
        compiler_params=pltpu.CompilerParams(vmem_limit_bytes=8 * MIB),
        cost_estimate=pl.CostEstimate(
            flops=2 * 128 * 24 * half, bytes_accessed=MIB, transcendentals=0
        ),
        name="combine",
    )(weights, first, second, *backs)


def per_device(tokens, cotangent, routes, route_weights, gate_weight, up_weight, down_weight):
    place = jnp.stack([lax.axis_index("core"), lax.axis_index("z"), lax.axis_index("yh")])
    place = place.astype(jnp.int32)
    offsets = [(dz, dy) for dz in range(4) for dy in range(2)]
    packed = EXPERTS * CAP
    third = packed // 3

    made = make_slots(place, tokens, cotangent, routes, route_weights)
    first, second = made[EXPERTS:]
    pieces = [made[0]] + [to_expert(made[k], *offsets[k], 1) for k in range(1, EXPERTS)]
    row_of = jnp.arange(packed)
    pack = (
        (row_of // CAP * ROOM + row_of % CAP)[:, None] == jnp.arange(EXPERTS * ROOM)[None, :]
    ).astype(BF)
    own = dot_f32(pack, jnp.concatenate(pieces, axis=0), 1, 0).astype(BF)

    left = along_x(own, 1)
    right = along_x(own, -1)
    partner = pair_y(own)
    far_left = along_x(partner, 1)
    far_right = pair_y(right)
    across = along_x(right, -1)

    gate_t = gate_weight[0].T
    up_t = up_weight[0].T
    down_t = down_weight[0]
    near = [own, left, right, partner]
    near_other = [pair_core(v) for v in near]
    near_out = run_group(place, near, near_other, gate_t, up_t, down_t)
    tied = lax.optimization_barrier((far_left, far_right, across, *near_out))
    far_left, far_right, across = tied[:3]
    near_out = tied[3:]
    last = [
        along_x(far_left[:third], 1),
        along_x(far_right[third : 2 * third], -1),
        pair_y(across[2 * third :]),
    ]

    far = [far_left, far_right, across] + last
    far_other = [pair_core(v) for v in far]
    far_out = run_group(place, far, far_other, gate_t, up_t, down_t)

    def add(a, *more):
        total = a.astype(F32)
        for m in more:
            total = total + m.astype(F32)
        return total.astype(BF)

    near_got = pair_core(near_out[1])
    far_got = pair_core(far_out[1])

    def chunk(out, got, i, a=0, b=packed):
        return add(out[0][packed * i + a : packed * i + b], got[packed * i + a : packed * i + b])

    t_last = [chunk(far_out, far_got, 3, third * i, third * (i + 1)) for i in range(3)]
    a_left = along_x(t_last[0], -1)
    a_right = along_x(t_last[1], 1)
    a_pair = pair_y(t_last[2])
    pads = [[(third * i, packed - third * (i + 1)), (0, 0)] for i in range(3)]
    t_far_left = add(chunk(far_out, far_got, 0), jnp.pad(a_left, pads[0]))
    t_far_right = add(chunk(far_out, far_got, 1), jnp.pad(a_right, pads[1]))
    t_across = add(chunk(far_out, far_got, 2), jnp.pad(a_pair, pads[2]))
    b_partner = along_x(t_far_left, -1)
    b_right_pair = pair_y(t_far_right)
    b_right = along_x(t_across, 1)
    ours, theirs = near + far, near_other + far_other
    half = tokens.shape[1] // 2
    gate_grad, up_grad = weight_grads(
        place, ours, theirs, [(near_out[2], far_out[2]), (near_out[3], far_out[3])], 0
    )
    b_partner, b_right_pair, b_right, gate_grad, up_grad = lax.optimization_barrier(
        (b_partner, b_right_pair, b_right, gate_grad, up_grad)
    )
    c_left = along_x(chunk(near_out, near_got, 1), -1)
    c_right = along_x(add(chunk(near_out, near_got, 2), b_right_pair, b_right), 1)
    c_pair = pair_y(add(chunk(near_out, near_got, 3), b_partner))
    (down_grad,) = weight_grads(place, ours, theirs, [(near_out[4], far_out[4])], half)
    c_left, c_right, c_pair, down_grad = lax.optimization_barrier(
        (c_left, c_right, c_pair, down_grad)
    )
    home = add(chunk(near_out, near_got, 0), c_left, c_right, c_pair)

    spread = dot_f32(pack, home, 0, 0).astype(BF)
    backs = [spread[:ROOM]] + [
        to_expert(spread[ROOM * k : ROOM * (k + 1)], *offsets[k], -1) for k in range(1, EXPERTS)
    ]
    token_grad, route_grad = combine(route_weights, first, second, backs)

    return token_grad, route_grad, gate_grad.T[None], up_grad.T[None], down_grad[None]


def solution(mesh):
    names = ("z", "yh", "yl", "x", "core")
    fine = Mesh(mesh.devices.reshape(4, 2, 2, 4, 2), names)
    ep = names[:4]
    return jax.shard_map(
        per_device,
        mesh=fine,
        in_specs=(
            P(ep, None),
            P(ep, None),
            P(ep, None),
            P(ep, None),
            P(ep, None, "core"),
            P(ep, None, "core"),
            P(ep, "core", None),
        ),
        out_specs=(
            P(ep, "core"),
            P(ep, None),
            P(ep, None, "core"),
            P(ep, None, "core"),
            P(ep, "core", None),
        ),
        check_vma=False,
    )
```

```python
import functools

import jax
import jax.numpy as jnp
from jax import lax
from jax.experimental import pallas as pl
from jax.experimental.pallas import tpu as pltpu
from jax.sharding import Mesh
from jax.sharding import PartitionSpec as P


EXPERTS = 8
TOP = 2
CAP = 12
ROOM = 16
LANES = 128
BF = jnp.bfloat16
F32 = jnp.float32
MIB = 1 << 20


VMEM = pl.BlockSpec(memory_space=pltpu.VMEM)
SMEM = pl.BlockSpec(memory_space=pltpu.SMEM)


def along_x(value, step):
    return lax.ppermute(value, "x", [(i, (i + step) % 4) for i in range(4)])


def pair_y(value):
    return lax.ppermute(value, "yl", [(0, 1), (1, 0)])


def pair_core(value):
    return lax.ppermute(value, "core", [(0, 1), (1, 0)])


def to_expert(value, dz, dy, sign):
    perm = []
    for z in range(4):
        for y in range(4):
            there = (z + sign * dz) % 4 * 4 + (3 - y if dy else y)
            perm.append((z * 4 + y, there))
    return lax.ppermute(value, ("z", "yh", "yl"), perm)


def dot_f32(a, b, left, right):
    return lax.dot_general(a, b, (((left,), (right,)), ((), ())), preferred_element_type=F32)


def slots_kernel(half, place_ref, tok_ref, cot_ref, routes_ref, weights_ref, *outs):
    core, z, yh = place_ref[0], place_ref[1], place_ref[2]
    first_ref, second_ref = outs[EXPERTS:]
    rows = tok_ref.shape[0]
    slot = lax.broadcasted_iota(jnp.int32, (rows, EXPERTS * ROOM), 1)
    index = slot // ROOM
    expert = 2 * ((z + index // 2) % 4) + (yh + index % 2) % 2
    is_first = routes_ref[:, 0:1] == expert
    is_second = routes_ref[:, 1:2] == expert
    hot = jnp.where(is_first | is_second, 1.0, 0.0).astype(BF)
    below = lax.broadcasted_iota(jnp.int32, (rows, rows), 1) < lax.broadcasted_iota(
        jnp.int32, (rows, rows), 0
    )
    position = dot_f32(jnp.where(below, 1.0, 0.0).astype(BF), hot, 1, 0)
    fits = position == (slot % ROOM).astype(F32)
    first = jnp.where(is_first & fits, 1.0, 0.0).astype(BF)
    second = jnp.where(is_second & fits, 1.0, 0.0).astype(BF)
    first_ref[...] = first
    second_ref[...] = second
    here = pl.ds(pl.multiple_of(core * half, half), half)
    slot_tok = dot_f32(first + second, tok_ref[:, here], 0, 0).astype(BF)
    cot = cot_ref[:, here].astype(F32)
    scaled = dot_f32(first, (cot * weights_ref[:, 0:1]).astype(BF), 0, 0)
    scaled = scaled + dot_f32(second, (cot * weights_ref[:, 1:2]).astype(BF), 0, 0)
    scaled = scaled.astype(BF)
    for k in range(EXPERTS):
        outs[k][:, :half] = slot_tok[k * ROOM : (k + 1) * ROOM]
        outs[k][:, half:] = scaled[k * ROOM : (k + 1) * ROOM]


def make_slots(place, tokens, cotangent, routes, weights):
    rows, width = tokens.shape
    shapes = [jax.ShapeDtypeStruct((ROOM, width), BF)] * EXPERTS
    shapes += [jax.ShapeDtypeStruct((rows, EXPERTS * ROOM), BF)] * 2
    return pl.pallas_call(
        functools.partial(slots_kernel, width // 2),
        out_shape=shapes,
        in_specs=[SMEM] + [VMEM] * 4,
        out_specs=[VMEM] * len(shapes),
        compiler_params=pltpu.CompilerParams(vmem_limit_bytes=8 * MIB),
        cost_estimate=pl.CostEstimate(
            flops=2 * 128 * 24 * width * 2, bytes_accessed=3 * MIB, transcendentals=0
        ),
        name="slots",
    )(place, tokens, cotangent, routes, weights)


def group_kernel(count, half, place_ref, *refs):
    core = place_ref[0]
    ours, theirs = refs[:count], refs[count : 2 * count]
    gate_ref, up_ref, down_ref = refs[2 * count : 2 * count + 3]
    keep_ref, send_ref, gate_out, up_out, hidden_out = refs[2 * count + 3 :]
    here = pl.ds(pl.multiple_of(core * half, half), half)
    there = pl.ds(pl.multiple_of((1 - core) * half, half), half)
    tok = [jnp.concatenate([r[:, :half] for r in side], axis=0) for side in (ours, theirs)]
    gate = dot_f32(tok[0], gate_ref[:, here], 1, 1) + dot_f32(tok[1], gate_ref[:, there], 1, 1)
    up = dot_f32(tok[0], up_ref[:, here], 1, 1) + dot_f32(tok[1], up_ref[:, there], 1, 1)
    cot = [jnp.concatenate([r[:, half:] for r in side], axis=0) for side in (ours, theirs)]
    grad = dot_f32(cot[0], down_ref[:, here], 1, 1) + dot_f32(cot[1], down_ref[:, there], 1, 1)
    sigma = 1.0 / (1.0 + jnp.exp(-gate))
    active = gate * sigma
    hidden = (active * up).astype(BF)
    gate_side = (grad * up * (sigma * (1.0 + gate * (1.0 - sigma)))).astype(BF)
    up_side = (grad * active).astype(BF)
    hidden_out[...] = hidden
    gate_out[...] = gate_side
    up_out[...] = up_side
    share = jnp.sum(hidden.astype(F32) * grad, axis=1, keepdims=True).astype(BF)
    share = jnp.broadcast_to(share, (share.shape[0], LANES))
    for where, out in ((here, keep_ref), (there, send_ref)):
        term = dot_f32(gate_side, gate_ref[:, where], 1, 0)
        term = term + dot_f32(up_side, up_ref[:, where], 1, 0)
        out[:, :half] = term.astype(BF)
        out[:, half:] = share


def run_group(place, ours, theirs, gate, up, down):
    rows = sum(r.shape[0] for r in ours)
    hid, width = gate.shape
    half = width // 2
    shapes = [jax.ShapeDtypeStruct((rows, half + LANES), BF)] * 2
    shapes += [jax.ShapeDtypeStruct((rows, hid), BF)] * 3
    return pl.pallas_call(
        functools.partial(group_kernel, len(ours), half),
        out_shape=shapes,
        in_specs=[SMEM] + [VMEM] * (2 * len(ours) + 3),
        out_specs=[VMEM] * len(shapes),
        compiler_params=pltpu.CompilerParams(vmem_limit_bytes=40 * MIB),
        cost_estimate=pl.CostEstimate(
            flops=10 * rows * hid * width, bytes_accessed=16 * MIB, transcendentals=rows * hid
        ),
        name="group",
    )(place, *ours, *theirs, gate, up, down)


def weight_kernel(count, half, offset, sides, place_ref, *refs):
    core = place_ref[0]
    ours, theirs = refs[:count], refs[count : 2 * count]
    side_refs = refs[2 * count : 2 * count + 2 * sides]
    outs = refs[2 * count + 2 * sides :]
    here = pl.ds(pl.multiple_of(core * half, half), half)
    there = pl.ds(pl.multiple_of((1 - core) * half, half), half)
    for group, where in ((ours, here), (theirs, there)):
        block = jnp.concatenate([r[:, offset : offset + half] for r in group], axis=0)
        for i in range(sides):
            side = jnp.concatenate([side_refs[2 * i][...], side_refs[2 * i + 1][...]], axis=0)
            outs[i][:, where] = dot_f32(side, block, 0, 0).astype(BF)


def weight_grads(place, ours, theirs, side_pairs, offset):
    rows = sum(r.shape[0] for r in ours)
    hid = side_pairs[0][0].shape[1]
    width = ours[0].shape[1]
    shapes = [jax.ShapeDtypeStruct((hid, width), BF)] * len(side_pairs)
    flat = [s for pair in side_pairs for s in pair]
    return pl.pallas_call(
        functools.partial(weight_kernel, len(ours), width // 2, offset, len(side_pairs)),
        out_shape=shapes,
        in_specs=[SMEM] + [VMEM] * (2 * len(ours) + len(flat)),
        out_specs=[VMEM] * len(shapes),
        compiler_params=pltpu.CompilerParams(vmem_limit_bytes=52 * MIB),
        cost_estimate=pl.CostEstimate(
            flops=2 * rows * hid * width * len(side_pairs),
            bytes_accessed=16 * MIB,
            transcendentals=0,
        ),
        name="weight_grads",
    )(place, *ours, *theirs, *flat)


def final_kernel(half, weights_ref, first_ref, second_ref, *refs):
    backs = refs[:EXPERTS]
    token_ref, route_ref = refs[EXPERTS:]
    back = jnp.concatenate([b[...] for b in backs], axis=0)
    first, second = first_ref[...], second_ref[...]
    token_ref[...] = dot_f32(first + second, back[:, :half], 1, 0).astype(BF)
    share = back[:, half:]
    route_ref[:, 0:1] = dot_f32(first, share, 1, 0)[:, 0:1] / weights_ref[:, 0:1]
    route_ref[:, 1:2] = dot_f32(second, share, 1, 0)[:, 0:1] / weights_ref[:, 1:2]


def combine(weights, first, second, backs):
    rows = weights.shape[0]
    half = backs[0].shape[1] - LANES
    return pl.pallas_call(
        functools.partial(final_kernel, half),
        out_shape=[
            jax.ShapeDtypeStruct((rows, half), BF),
            jax.ShapeDtypeStruct((rows, TOP), F32),
        ],
        in_specs=[VMEM] * (3 + EXPERTS),
        out_specs=[VMEM] * 2,
        compiler_params=pltpu.CompilerParams(vmem_limit_bytes=8 * MIB),
        cost_estimate=pl.CostEstimate(
            flops=2 * 128 * 24 * half, bytes_accessed=MIB, transcendentals=0
        ),
        name="combine",
    )(weights, first, second, *backs)


def per_device(tokens, cotangent, routes, route_weights, gate_weight, up_weight, down_weight):
    place = jnp.stack([lax.axis_index("core"), lax.axis_index("z"), lax.axis_index("yh")])
    place = place.astype(jnp.int32)
    packed = EXPERTS * CAP
    third = packed // 3

    made = make_slots(place, tokens, cotangent, routes, route_weights)
    first, second = made[EXPERTS:]
    part = packed // 2
    row_of = jnp.arange(part)
    pack = (
        (row_of // CAP * ROOM + row_of % CAP)[:, None] == jnp.arange(EXPERTS * ROOM // 2)[None, :]
    ).astype(BF)

    def packing(sent, dy):
        got = list(sent)
        for dz in (2, 1, 3, 0):
            if dz or dy:
                got[dz] = to_expert(sent[dz], dz, dy, 1)
        return dot_f32(pack, jnp.concatenate(got, axis=0), 1, 0).astype(BF)

    own, left, right, partner, far_left, far_right, across = ([] for _ in range(7))
    own.append(packing(made[0:EXPERTS:2], 0))
    tied = lax.optimization_barrier((own[0], *made[1:EXPERTS:2]))
    own = [tied[0], packing(tied[1:], 1)]
    for h in range(2):
        left.append(along_x(own[h], 1))
        right.append(along_x(own[h], -1))
        partner.append(pair_y(own[h]))
    for h in range(2):
        far_left.append(along_x(partner[h], 1))
        far_right.append(pair_y(right[h]))
        across.append(along_x(right[h], -1))

    gate_t = gate_weight[0].T
    up_t = up_weight[0].T
    down_t = down_weight[0]
    near = own + left + right + partner
    near_other = [pair_core(v) for v in near]
    near_out = run_group(place, near, near_other, gate_t, up_t, down_t)
    far = far_left + far_right + across
    tied = lax.optimization_barrier((*far, *near_out))
    far = list(tied[: len(far)])
    near_out = tied[len(far) :]
    middle = jnp.concatenate([far[2][third:], far[3][: 2 * third - part]], axis=0)
    last = [along_x(far[0][:third], 1), along_x(middle, -1), pair_y(far[5][2 * third - part :])]
    far = far + last
    far_other = [pair_core(v) for v in far]
    far_out = run_group(place, far, far_other, gate_t, up_t, down_t)

    def add(a, *more):
        total = a.astype(F32)
        for m in more:
            total = total + m.astype(F32)
        return total.astype(BF)

    near_got = pair_core(near_out[1])
    far_got = pair_core(far_out[1])

    def chunk(out, got, i, a=0, b=packed):
        return add(out[0][packed * i + a : packed * i + b], got[packed * i + a : packed * i + b])

    t_last = [chunk(far_out, far_got, 3, third * i, third * (i + 1)) for i in range(3)]
    a_left = along_x(t_last[0], -1)
    a_right = along_x(t_last[1], 1)
    a_pair = pair_y(t_last[2])
    pads = [[(third * i, packed - third * (i + 1)), (0, 0)] for i in range(3)]
    t_far_left = add(chunk(far_out, far_got, 0), jnp.pad(a_left, pads[0]))
    t_far_right = add(chunk(far_out, far_got, 1), jnp.pad(a_right, pads[1]))
    t_across = add(chunk(far_out, far_got, 2), jnp.pad(a_pair, pads[2]))
    b_partner = along_x(t_far_left, -1)
    b_right_pair = pair_y(t_far_right)
    b_right = along_x(t_across, 1)
    ours, theirs = near + far, near_other + far_other
    half = tokens.shape[1] // 2
    gate_grad, up_grad = weight_grads(
        place, ours, theirs, [(near_out[2], far_out[2]), (near_out[3], far_out[3])], 0
    )
    b_partner, b_right_pair, b_right, gate_grad, up_grad = lax.optimization_barrier(
        (b_partner, b_right_pair, b_right, gate_grad, up_grad)
    )
    c_left = along_x(chunk(near_out, near_got, 1), -1)
    c_right = along_x(add(chunk(near_out, near_got, 2), b_right_pair, b_right), 1)
    c_pair = pair_y(add(chunk(near_out, near_got, 3), b_partner))
    (down_grad,) = weight_grads(place, ours, theirs, [(near_out[4], far_out[4])], half)
    c_left, c_right, c_pair, down_grad = lax.optimization_barrier(
        (c_left, c_right, c_pair, down_grad)
    )
    home = add(chunk(near_out, near_got, 0), c_left, c_right, c_pair)

    backs = [None] * EXPERTS
    for dy in range(2):
        spread = dot_f32(pack, home[part * dy : part * (dy + 1)], 0, 0).astype(BF)
        for dz in (2, 1, 3, 0):
            k = 2 * dz + dy
            piece = spread[ROOM * dz : ROOM * (dz + 1)]
            if k:
                piece = to_expert(piece, dz, dy, -1)
            backs[k] = piece
    token_grad, route_grad = combine(route_weights, first, second, backs)

    return token_grad, route_grad, gate_grad.T[None], up_grad.T[None], down_grad[None]


def solution(mesh):
    names = ("z", "yh", "yl", "x", "core")
    fine = Mesh(mesh.devices.reshape(4, 2, 2, 4, 2), names)
    ep = names[:4]
    return jax.shard_map(
        per_device,
        mesh=fine,
        in_specs=(
            P(ep, None),
            P(ep, None),
            P(ep, None),
            P(ep, None),
            P(ep, None, "core"),
            P(ep, None, "core"),
            P(ep, "core", None),
        ),
        out_specs=(
            P(ep, "core"),
            P(ep, None),
            P(ep, None, "core"),
            P(ep, None, "core"),
            P(ep, "core", None),
        ),
        check_vma=False,
    )
```

```python
import functools

import jax
import jax.numpy as jnp
from jax import lax
from jax.experimental import pallas as pl
from jax.experimental.pallas import tpu as pltpu
from jax.sharding import Mesh
from jax.sharding import PartitionSpec as P


EXPERTS = 8
TOP = 2
CAP = 12
ROOM = 16
LANES = 128
BF = jnp.bfloat16
F32 = jnp.float32
MIB = 1 << 20


VMEM = pl.BlockSpec(memory_space=pltpu.VMEM)
SMEM = pl.BlockSpec(memory_space=pltpu.SMEM)


def along_x(value, step):
    return lax.ppermute(value, "x", [(i, (i + step) % 4) for i in range(4)])


def pair_y(value):
    return lax.ppermute(value, "yl", [(0, 1), (1, 0)])


def pair_core(value):
    return lax.ppermute(value, "core", [(0, 1), (1, 0)])


def to_expert(value, dz, dy, sign):
    perm = []
    for z in range(4):
        for y in range(4):
            there = (z + sign * dz) % 4 * 4 + (3 - y if dy else y)
            perm.append((z * 4 + y, there))
    return lax.ppermute(value, ("z", "yh", "yl"), perm)


def dot_f32(a, b, left, right):
    return lax.dot_general(a, b, (((left,), (right,)), ((), ())), preferred_element_type=F32)


def slots_kernel(half, place_ref, tok_ref, cot_ref, routes_ref, weights_ref, *outs):
    core, z, yh = place_ref[0], place_ref[1], place_ref[2]
    first_ref, second_ref = outs[EXPERTS:]
    rows = tok_ref.shape[0]
    slot = lax.broadcasted_iota(jnp.int32, (rows, EXPERTS * ROOM), 1)
    index = slot // ROOM
    expert = 2 * ((z + index // 2) % 4) + (yh + index % 2) % 2
    is_first = routes_ref[:, 0:1] == expert
    is_second = routes_ref[:, 1:2] == expert
    hot = jnp.where(is_first | is_second, 1.0, 0.0).astype(BF)
    below = lax.broadcasted_iota(jnp.int32, (rows, rows), 1) < lax.broadcasted_iota(
        jnp.int32, (rows, rows), 0
    )
    position = dot_f32(jnp.where(below, 1.0, 0.0).astype(BF), hot, 1, 0)
    fits = position == (slot % ROOM).astype(F32)
    first = jnp.where(is_first & fits, 1.0, 0.0).astype(BF)
    second = jnp.where(is_second & fits, 1.0, 0.0).astype(BF)
    first_ref[...] = first
    second_ref[...] = second
    here = pl.ds(pl.multiple_of(core * half, half), half)
    slot_tok = dot_f32(first + second, tok_ref[:, here], 0, 0).astype(BF)
    cot = cot_ref[:, here].astype(F32)
    scaled = dot_f32(first, (cot * weights_ref[:, 0:1]).astype(BF), 0, 0)
    scaled = scaled + dot_f32(second, (cot * weights_ref[:, 1:2]).astype(BF), 0, 0)
    scaled = scaled.astype(BF)
    for k in range(EXPERTS):
        outs[k][:, :half] = slot_tok[k * ROOM : (k + 1) * ROOM]
        outs[k][:, half:] = scaled[k * ROOM : (k + 1) * ROOM]


def make_slots(place, tokens, cotangent, routes, weights):
    rows, width = tokens.shape
    shapes = [jax.ShapeDtypeStruct((ROOM, width), BF)] * EXPERTS
    shapes += [jax.ShapeDtypeStruct((rows, EXPERTS * ROOM), BF)] * 2
    return pl.pallas_call(
        functools.partial(slots_kernel, width // 2),
        out_shape=shapes,
        in_specs=[SMEM] + [VMEM] * 4,
        out_specs=[VMEM] * len(shapes),
        compiler_params=pltpu.CompilerParams(vmem_limit_bytes=8 * MIB),
        cost_estimate=pl.CostEstimate(
            flops=2 * 128 * 24 * width * 2, bytes_accessed=3 * MIB, transcendentals=0
        ),
        name="slots",
    )(place, tokens, cotangent, routes, weights)


def padded(n):
    return -(-n // LANES) * LANES


def group_kernel(count, half, place_ref, *refs):
    core = place_ref[0]
    ours, theirs = refs[:count], refs[count : 2 * count]
    gate_ref, up_ref, down_ref = refs[2 * count : 2 * count + 3]
    keep_ref, send_ref, gate_out, up_out, hidden_out = refs[2 * count + 3 :]
    here = pl.ds(pl.multiple_of(core * half, half), half)
    there = pl.ds(pl.multiple_of((1 - core) * half, half), half)
    tok = [jnp.concatenate([r[:, :half] for r in side], axis=0) for side in (ours, theirs)]
    gate = dot_f32(tok[0], gate_ref[:, here], 1, 1) + dot_f32(tok[1], gate_ref[:, there], 1, 1)
    up = dot_f32(tok[0], up_ref[:, here], 1, 1) + dot_f32(tok[1], up_ref[:, there], 1, 1)
    cot = [jnp.concatenate([r[:, half:] for r in side], axis=0) for side in (ours, theirs)]
    grad = dot_f32(cot[0], down_ref[:, here], 1, 1) + dot_f32(cot[1], down_ref[:, there], 1, 1)
    sigma = 1.0 / (1.0 + jnp.exp(-gate))
    active = gate * sigma
    hidden = (active * up).astype(BF)
    gate_side = (grad * up * (sigma * (1.0 + gate * (1.0 - sigma)))).astype(BF)
    up_side = (grad * active).astype(BF)
    hid = hidden.shape[1]
    for out, value in ((hidden_out, hidden), (gate_out, gate_side), (up_out, up_side)):
        out[:, :hid] = value
        out[:, hid:] = jnp.zeros((out.shape[0], out.shape[1] - hid), BF)
    share = jnp.sum(hidden.astype(F32) * grad, axis=1, keepdims=True).astype(BF)
    share = jnp.broadcast_to(share, (share.shape[0], LANES))
    tile = 512
    for base, out in ((core * half, keep_ref), ((1 - core) * half, send_ref)):
        out[:, half:] = share

        @pl.loop(0, half // tile)
        def _(j):
            where = pl.ds(pl.multiple_of(base + j * tile, tile), tile)
            term = dot_f32(gate_out[:, :hid], gate_ref[:, where], 1, 0)
            term = term + dot_f32(up_out[:, :hid], up_ref[:, where], 1, 0)
            out[:, pl.ds(pl.multiple_of(j * tile, tile), tile)] = term.astype(BF)


def run_group(place, ours, theirs, gate, up, down):
    rows = sum(r.shape[0] for r in ours)
    hid, width = gate.shape
    half = width // 2
    shapes = [jax.ShapeDtypeStruct((rows, half + LANES), BF)] * 2
    shapes += [jax.ShapeDtypeStruct((rows, padded(hid)), BF)] * 3
    return pl.pallas_call(
        functools.partial(group_kernel, len(ours), half),
        out_shape=shapes,
        in_specs=[SMEM] + [VMEM] * (2 * len(ours) + 3),
        out_specs=[VMEM] * len(shapes),
        compiler_params=pltpu.CompilerParams(vmem_limit_bytes=40 * MIB),
        cost_estimate=pl.CostEstimate(
            flops=10 * rows * hid * width, bytes_accessed=16 * MIB, transcendentals=rows * hid
        ),
        name="group",
    )(place, *ours, *theirs, gate, up, down)


def weight_kernel(sizes, half, hid, tile, place_ref, *refs):
    count = len(sizes)
    ours, theirs = refs[:count], refs[count : 2 * count]
    sides = refs[2 * count : 2 * count + 6]
    outs = refs[2 * count + 6 : 2 * count + 9]
    rows_ref, pair_t, hidden_t, stage, in_sem, out_sem = refs[2 * count + 9 :]
    core = place_ref[0]
    loads = []
    for s, group in enumerate((ours, theirs)):
        at = 0
        copies = []
        for i, size in enumerate(sizes):
            copies.append(
                pltpu.make_async_copy(
                    group[i], rows_ref.at[s, pl.ds(at, size), :], in_sem.at[s, i]
                )
            )
            at += size
        loads.append(copies)
    for copies in loads:
        for c in copies:
            c.start()
    wide = sides[0].shape[1]
    depth = sides[0].shape[0]
    for i in range(2):
        columns = slice(depth * i, depth * (i + 1))
        pair_t[:wide, columns] = sides[i][...].T
        pair_t[wide:, columns] = sides[2 + i][...].T
        hidden_t[:, columns] = sides[4 + i][...].T
    stores = []
    for s in range(2):
        for c in loads[s]:
            c.wait()
        base = (core if s == 0 else 1 - core) * half

        @pl.loop(0, half // tile)
        def _(j):
            to = pl.ds(pl.multiple_of(base + j * tile, tile), tile)
            block = rows_ref[s, :, pl.ds(pl.multiple_of(j * tile, tile), tile)]
            pair = dot_f32(pair_t[...], block, 1, 0).astype(BF)
            stage[0, :, to] = pair[:hid]
            stage[1, :, to] = pair[wide : wide + hid]
            block = rows_ref[s, :, pl.ds(pl.multiple_of(half + j * tile, tile), tile)]
            stage[2, :, to] = dot_f32(hidden_t[...], block, 1, 0).astype(BF)[:hid]

        whole = pl.ds(pl.multiple_of(base, half), half)
        for t in range(3):
            copy = pltpu.make_async_copy(
                stage.at[t, :, whole], outs[t].at[:, whole], out_sem.at[s, t]
            )
            copy.start()
            stores.append(copy)
    for copy in stores:
        copy.wait()


def weight_grads(place, ours, theirs, sides, hid):
    sizes = [r.shape[0] for r in ours]
    rows = sum(sizes)
    width = ours[0].shape[1]
    wide = sides[0].shape[1]
    anywhere = pl.BlockSpec(memory_space=pl.ANY)
    return pl.pallas_call(
        functools.partial(weight_kernel, sizes, width // 2, hid, 512),
        out_shape=[jax.ShapeDtypeStruct((hid, width), BF)] * 3,
        in_specs=[SMEM] + [anywhere] * (2 * len(sizes)) + [VMEM] * 6,
        out_specs=[anywhere] * 3,
        scratch_shapes=[
            pltpu.VMEM((2, rows, width), BF),
            pltpu.VMEM((2 * wide, rows), BF),
            pltpu.VMEM((wide, rows), BF),
            pltpu.VMEM((3, hid, width), BF),
            pltpu.SemaphoreType.DMA((2, len(sizes))),
            pltpu.SemaphoreType.DMA((2, 3)),
        ],
        compiler_params=pltpu.CompilerParams(vmem_limit_bytes=36 * MIB),
        cost_estimate=pl.CostEstimate(
            flops=6 * rows * hid * width, bytes_accessed=22 * MIB, transcendentals=0
        ),
        name="weight_grads",
    )(place, *ours, *theirs, *sides)


def final_kernel(half, weights_ref, first_ref, second_ref, *refs):
    backs = refs[:EXPERTS]
    token_ref, route_ref = refs[EXPERTS:]
    back = jnp.concatenate([b[...] for b in backs], axis=0)
    first, second = first_ref[...], second_ref[...]
    token_ref[...] = dot_f32(first + second, back[:, :half], 1, 0).astype(BF)
    share = back[:, half:]
    route_ref[:, 0:1] = dot_f32(first, share, 1, 0)[:, 0:1] / weights_ref[:, 0:1]
    route_ref[:, 1:2] = dot_f32(second, share, 1, 0)[:, 0:1] / weights_ref[:, 1:2]


def combine(weights, first, second, backs):
    rows = weights.shape[0]
    half = backs[0].shape[1] - LANES
    return pl.pallas_call(
        functools.partial(final_kernel, half),
        out_shape=[
            jax.ShapeDtypeStruct((rows, half), BF),
            jax.ShapeDtypeStruct((rows, TOP), F32),
        ],
        in_specs=[VMEM] * (3 + EXPERTS),
        out_specs=[VMEM] * 2,
        compiler_params=pltpu.CompilerParams(vmem_limit_bytes=8 * MIB),
        cost_estimate=pl.CostEstimate(
            flops=2 * 128 * 24 * half, bytes_accessed=MIB, transcendentals=0
        ),
        name="combine",
    )(weights, first, second, *backs)


def per_device(tokens, cotangent, routes, route_weights, gate_weight, up_weight, down_weight):
    place = jnp.stack([lax.axis_index("core"), lax.axis_index("z"), lax.axis_index("yh")])
    place = place.astype(jnp.int32)
    packed = EXPERTS * CAP
    third = packed // 3

    made = make_slots(place, tokens, cotangent, routes, route_weights)
    first, second = made[EXPERTS:]
    part = packed // 2
    row_of = jnp.arange(part)
    pack = (
        (row_of // CAP * ROOM + row_of % CAP)[:, None] == jnp.arange(EXPERTS * ROOM // 2)[None, :]
    ).astype(BF)

    def packing(sent, dy):
        got = list(sent)
        for dz in (2, 1, 3, 0):
            if dz or dy:
                got[dz] = to_expert(sent[dz], dz, dy, 1)
        return dot_f32(pack, jnp.concatenate(got, axis=0), 1, 0).astype(BF)

    own, left, right, partner, far_left, far_right, across = ([] for _ in range(7))
    own = [packing(made[h:EXPERTS:2], h) for h in range(2)]
    for h in range(2):
        left.append(along_x(own[h], 1))
        right.append(along_x(own[h], -1))
        partner.append(pair_y(own[h]))
    for h in range(2):
        far_left.append(along_x(partner[h], 1))
        far_right.append(pair_y(right[h]))
        across.append(along_x(right[h], -1))

    gate_t = gate_weight[0].T
    up_t = up_weight[0].T
    down_t = down_weight[0]
    near = own + left + right + partner
    near_other = [pair_core(v) for v in near]
    near_out = run_group(place, near, near_other, gate_t, up_t, down_t)
    far = far_left + far_right + across
    tied = lax.optimization_barrier((*far, *near_out))
    far = list(tied[: len(far)])
    near_out = tied[len(far) :]
    middle = jnp.concatenate([far[2][third:], far[3][: 2 * third - part]], axis=0)
    last = [along_x(far[0][:third], 1), along_x(middle, -1), pair_y(far[5][2 * third - part :])]
    far = far + last
    far_other = [pair_core(v) for v in far]
    far_out = run_group(place, far, far_other, gate_t, up_t, down_t)

    def add(a, *more):
        total = a.astype(F32)
        for m in more:
            total = total + m.astype(F32)
        return total.astype(BF)

    near_got = pair_core(near_out[1])
    far_got = pair_core(far_out[1])

    def chunk(out, got, i, a=0, b=packed):
        return add(out[0][packed * i + a : packed * i + b], got[packed * i + a : packed * i + b])

    t_last = [chunk(far_out, far_got, 3, third * i, third * (i + 1)) for i in range(3)]
    a_left = along_x(t_last[0], -1)
    a_right = along_x(t_last[1], 1)
    a_pair = pair_y(t_last[2])
    pads = [[(third * i, packed - third * (i + 1)), (0, 0)] for i in range(3)]
    t_far_left = add(chunk(far_out, far_got, 0), jnp.pad(a_left, pads[0]))
    t_far_right = add(chunk(far_out, far_got, 1), jnp.pad(a_right, pads[1]))
    t_across = add(chunk(far_out, far_got, 2), jnp.pad(a_pair, pads[2]))
    b_partner = along_x(t_far_left, -1)
    b_right_pair = pair_y(t_far_right)
    b_right = along_x(t_across, 1)
    hid = gate_t.shape[0]
    sides = [g for t in (2, 3, 4) for g in (near_out[t], far_out[t])]
    grads = weight_grads(place, near + far, near_other + far_other, sides, hid)
    tied = lax.optimization_barrier((b_partner, b_right_pair, b_right, *grads))
    b_partner, b_right_pair, b_right, gate_grad, up_grad, down_grad = tied
    c_left = along_x(chunk(near_out, near_got, 1), -1)
    c_right = along_x(add(chunk(near_out, near_got, 2), b_right_pair, b_right), 1)
    c_pair = pair_y(add(chunk(near_out, near_got, 3), b_partner))
    home = add(chunk(near_out, near_got, 0), c_left, c_right, c_pair)

    backs = [None] * EXPERTS
    for dy in range(2):
        spread = dot_f32(pack, home[part * dy : part * (dy + 1)], 0, 0).astype(BF)
        for dz in (2, 1, 3, 0):
            k = 2 * dz + dy
            piece = spread[ROOM * dz : ROOM * (dz + 1)]
            if k:
                piece = to_expert(piece, dz, dy, -1)
            backs[k] = piece
    token_grad, route_grad = combine(route_weights, first, second, backs)

    return token_grad, route_grad, gate_grad.T[None], up_grad.T[None], down_grad[None]


def solution(mesh):
    names = ("z", "yh", "yl", "x", "core")
    fine = Mesh(mesh.devices.reshape(4, 2, 2, 4, 2), names)
    ep = names[:4]
    return jax.shard_map(
        per_device,
        mesh=fine,
        in_specs=(
            P(ep, None),
            P(ep, None),
            P(ep, None),
            P(ep, None),
            P(ep, None, "core"),
            P(ep, None, "core"),
            P(ep, "core", None),
        ),
        out_specs=(
            P(ep, "core"),
            P(ep, None),
            P(ep, None, "core"),
            P(ep, None, "core"),
            P(ep, "core", None),
        ),
        check_vma=False,
    )
```

```python
import functools

import jax
import jax.numpy as jnp
from jax import lax
from jax.experimental import pallas as pl
from jax.experimental.pallas import tpu as pltpu
from jax.sharding import Mesh
from jax.sharding import PartitionSpec as P


EXPERTS = 8
TOP = 2
CAP = 12
ROOM = 16
LANES = 128
BF = jnp.bfloat16
F32 = jnp.float32
MIB = 1 << 20


VMEM = pl.BlockSpec(memory_space=pltpu.VMEM)
SMEM = pl.BlockSpec(memory_space=pltpu.SMEM)


def along_x(value, step):
    return lax.ppermute(value, "x", [(i, (i + step) % 4) for i in range(4)])


def pair_y(value):
    return lax.ppermute(value, "yl", [(0, 1), (1, 0)])


def pair_core(value):
    return lax.ppermute(value, "core", [(0, 1), (1, 0)])


def to_expert(value, dz, dy, sign):
    perm = []
    for z in range(4):
        for y in range(4):
            there = (z + sign * dz) % 4 * 4 + (3 - y if dy else y)
            perm.append((z * 4 + y, there))
    return lax.ppermute(value, ("z", "yh", "yl"), perm)


def dot_f32(a, b, left, right):
    return lax.dot_general(a, b, (((left,), (right,)), ((), ())), preferred_element_type=F32)


def slots_kernel(half, place_ref, tok_ref, cot_ref, routes_ref, weights_ref, *outs):
    core, z, yh = place_ref[0], place_ref[1], place_ref[2]
    first_ref, second_ref = outs[EXPERTS:]
    rows = tok_ref.shape[0]
    slot = lax.broadcasted_iota(jnp.int32, (rows, EXPERTS * ROOM), 1)
    index = slot // ROOM
    expert = 2 * ((z + index // 2) % 4) + (yh + index % 2) % 2
    is_first = routes_ref[:, 0:1] == expert
    is_second = routes_ref[:, 1:2] == expert
    hot = jnp.where(is_first | is_second, 1.0, 0.0).astype(BF)
    below = lax.broadcasted_iota(jnp.int32, (rows, rows), 1) < lax.broadcasted_iota(
        jnp.int32, (rows, rows), 0
    )
    position = dot_f32(jnp.where(below, 1.0, 0.0).astype(BF), hot, 1, 0)
    fits = position == (slot % ROOM).astype(F32)
    first = jnp.where(is_first & fits, 1.0, 0.0).astype(BF)
    second = jnp.where(is_second & fits, 1.0, 0.0).astype(BF)
    first_ref[...] = first
    second_ref[...] = second
    here = pl.ds(pl.multiple_of(core * half, half), half)
    slot_tok = dot_f32(first + second, tok_ref[:, here], 0, 0).astype(BF)
    cot = cot_ref[:, here].astype(F32)
    scaled = dot_f32(first, (cot * weights_ref[:, 0:1]).astype(BF), 0, 0)
    scaled = scaled + dot_f32(second, (cot * weights_ref[:, 1:2]).astype(BF), 0, 0)
    scaled = scaled.astype(BF)
    for k in range(EXPERTS):
        outs[k][:, :half] = slot_tok[k * ROOM : (k + 1) * ROOM]
        outs[k][:, half:] = scaled[k * ROOM : (k + 1) * ROOM]


def make_slots(place, tokens, cotangent, routes, weights):
    rows, width = tokens.shape
    shapes = [jax.ShapeDtypeStruct((ROOM, width), BF)] * EXPERTS
    shapes += [jax.ShapeDtypeStruct((rows, EXPERTS * ROOM), BF)] * 2
    return pl.pallas_call(
        functools.partial(slots_kernel, width // 2),
        out_shape=shapes,
        in_specs=[SMEM] + [VMEM] * 4,
        out_specs=[VMEM] * len(shapes),
        compiler_params=pltpu.CompilerParams(vmem_limit_bytes=8 * MIB),
        cost_estimate=pl.CostEstimate(
            flops=2 * 128 * 24 * width * 2, bytes_accessed=3 * MIB, transcendentals=0
        ),
        name="slots",
    )(place, tokens, cotangent, routes, weights)


def padded(n):
    return -(-n // LANES) * LANES


def group_kernel(count, half, place_ref, *refs):
    core = place_ref[0]
    ours, theirs = refs[:count], refs[count : 2 * count]
    gate_ref, up_ref, down_ref = refs[2 * count : 2 * count + 3]
    keep_ref, send_ref, gate_out, up_out, hidden_out = refs[2 * count + 3 :]
    here = pl.ds(pl.multiple_of(core * half, half), half)
    there = pl.ds(pl.multiple_of((1 - core) * half, half), half)
    tok = [jnp.concatenate([r[:, :half] for r in side], axis=0) for side in (ours, theirs)]
    gate = dot_f32(tok[0], gate_ref[:, here], 1, 1) + dot_f32(tok[1], gate_ref[:, there], 1, 1)
    up = dot_f32(tok[0], up_ref[:, here], 1, 1) + dot_f32(tok[1], up_ref[:, there], 1, 1)
    cot = [jnp.concatenate([r[:, half:] for r in side], axis=0) for side in (ours, theirs)]
    grad = dot_f32(cot[0], down_ref[:, here], 1, 1) + dot_f32(cot[1], down_ref[:, there], 1, 1)
    sigma = 1.0 / (1.0 + jnp.exp(-gate))
    active = gate * sigma
    hidden = (active * up).astype(BF)
    gate_side = (grad * up * (sigma * (1.0 + gate * (1.0 - sigma)))).astype(BF)
    up_side = (grad * active).astype(BF)
    hid = hidden.shape[1]
    for out, value in ((hidden_out, hidden), (gate_out, gate_side), (up_out, up_side)):
        out[:, :hid] = value
        out[:, hid:] = jnp.zeros((out.shape[0], out.shape[1] - hid), BF)
    share = jnp.sum(hidden.astype(F32) * grad, axis=1, keepdims=True).astype(BF)
    share = jnp.broadcast_to(share, (share.shape[0], LANES))
    tile = 512
    for base, out in ((core * half, keep_ref), ((1 - core) * half, send_ref)):
        out[:, half:] = share

        @pl.loop(0, half // tile)
        def _(j):
            where = pl.ds(pl.multiple_of(base + j * tile, tile), tile)
            term = dot_f32(gate_out[:, :hid], gate_ref[:, where], 1, 0)
            term = term + dot_f32(up_out[:, :hid], up_ref[:, where], 1, 0)
            out[:, pl.ds(pl.multiple_of(j * tile, tile), tile)] = term.astype(BF)


def run_group(place, ours, theirs, gate, up, down):
    rows = sum(r.shape[0] for r in ours)
    hid, width = gate.shape
    half = width // 2
    shapes = [jax.ShapeDtypeStruct((rows, half + LANES), BF)] * 2
    shapes += [jax.ShapeDtypeStruct((rows, padded(hid)), BF)] * 3
    return pl.pallas_call(
        functools.partial(group_kernel, len(ours), half),
        out_shape=shapes,
        in_specs=[SMEM] + [VMEM] * (2 * len(ours) + 3),
        out_specs=[VMEM] * len(shapes),
        compiler_params=pltpu.CompilerParams(vmem_limit_bytes=40 * MIB),
        cost_estimate=pl.CostEstimate(
            flops=10 * rows * hid * width, bytes_accessed=16 * MIB, transcendentals=rows * hid
        ),
        name="group",
    )(place, *ours, *theirs, gate, up, down)


def weight_kernel(sizes, offset, half, hid, tile, place_ref, *refs):
    count = len(sizes)
    kinds = (len(refs) - 2 * count - 5) // 3
    ours, theirs = refs[:count], refs[count : 2 * count]
    sides = refs[2 * count : 2 * count + 2 * kinds]
    outs = refs[2 * count + 2 * kinds : 2 * count + 3 * kinds]
    rows_ref, sides_t, stage, in_sem, out_sem = refs[2 * count + 3 * kinds :]
    core = place_ref[0]
    loads = []
    for s, group in enumerate((ours, theirs)):
        at = 0
        copies = []
        for i, size in enumerate(sizes):
            copies.append(
                pltpu.make_async_copy(
                    group[i].at[:, pl.ds(offset, half)],
                    rows_ref.at[s, pl.ds(at, size), :],
                    in_sem.at[s, i],
                )
            )
            at += size
        loads.append(copies)
    for copies in loads:
        for c in copies:
            c.start()
    depth, wide = sides[0].shape
    for k in range(kinds):
        for i in range(2):
            sides_t[wide * k : wide * (k + 1), depth * i : depth * (i + 1)] = sides[2 * k + i][...].T
    stores = []
    for s in range(2):
        for c in loads[s]:
            c.wait()
        base = (core if s == 0 else 1 - core) * half

        @pl.loop(0, half // tile)
        def _(j):
            to = pl.ds(pl.multiple_of(base + j * tile, tile), tile)
            block = rows_ref[s, :, pl.ds(pl.multiple_of(j * tile, tile), tile)]
            grads = dot_f32(sides_t[...], block, 1, 0).astype(BF)
            for k in range(kinds):
                stage[k, :, to] = grads[wide * k : wide * k + hid]

        whole = pl.ds(pl.multiple_of(base, half), half)
        for k in range(kinds):
            copy = pltpu.make_async_copy(
                stage.at[k, :, whole], outs[k].at[:, whole], out_sem.at[s, k]
            )
            copy.start()
            stores.append(copy)
    for copy in stores:
        copy.wait()


def weight_grads(place, ours, theirs, sides, offset, hid, tile=1024):
    sizes = [r.shape[0] for r in ours]
    rows = sum(sizes)
    width = ours[0].shape[1]
    wide = sides[0].shape[1]
    kinds = len(sides) // 2
    anywhere = pl.BlockSpec(memory_space=pl.ANY)
    return pl.pallas_call(
        functools.partial(weight_kernel, sizes, offset, width // 2, hid, tile),
        out_shape=[jax.ShapeDtypeStruct((hid, width), BF)] * kinds,
        in_specs=[SMEM] + [anywhere] * (2 * len(sizes)) + [VMEM] * len(sides),
        out_specs=[anywhere] * kinds,
        scratch_shapes=[
            pltpu.VMEM((2, rows, width // 2), BF),
            pltpu.VMEM((kinds * wide, rows), BF),
            pltpu.VMEM((kinds, hid, width), BF),
            pltpu.SemaphoreType.DMA((2, len(sizes))),
            pltpu.SemaphoreType.DMA((2, kinds)),
        ],
        compiler_params=pltpu.CompilerParams(vmem_limit_bytes=28 * MIB),
        cost_estimate=pl.CostEstimate(
            flops=2 * kinds * rows * hid * width, bytes_accessed=14 * MIB, transcendentals=0
        ),
        name="weight_grads",
    )(place, *ours, *theirs, *sides)


def final_kernel(half, weights_ref, first_ref, second_ref, *refs):
    backs = refs[:EXPERTS]
    token_ref, route_ref = refs[EXPERTS:]
    back = jnp.concatenate([b[...] for b in backs], axis=0)
    first, second = first_ref[...], second_ref[...]
    token_ref[...] = dot_f32(first + second, back[:, :half], 1, 0).astype(BF)
    share = back[:, half:]
    route_ref[:, 0:1] = dot_f32(first, share, 1, 0)[:, 0:1] / weights_ref[:, 0:1]
    route_ref[:, 1:2] = dot_f32(second, share, 1, 0)[:, 0:1] / weights_ref[:, 1:2]


def combine(weights, first, second, backs):
    rows = weights.shape[0]
    half = backs[0].shape[1] - LANES
    return pl.pallas_call(
        functools.partial(final_kernel, half),
        out_shape=[
            jax.ShapeDtypeStruct((rows, half), BF),
            jax.ShapeDtypeStruct((rows, TOP), F32),
        ],
        in_specs=[VMEM] * (3 + EXPERTS),
        out_specs=[VMEM] * 2,
        compiler_params=pltpu.CompilerParams(vmem_limit_bytes=8 * MIB),
        cost_estimate=pl.CostEstimate(
            flops=2 * 128 * 24 * half, bytes_accessed=MIB, transcendentals=0
        ),
        name="combine",
    )(weights, first, second, *backs)


def per_device(tokens, cotangent, routes, route_weights, gate_weight, up_weight, down_weight):
    place = jnp.stack([lax.axis_index("core"), lax.axis_index("z"), lax.axis_index("yh")])
    place = place.astype(jnp.int32)
    packed = EXPERTS * CAP
    third = packed // 3

    made = make_slots(place, tokens, cotangent, routes, route_weights)
    first, second = made[EXPERTS:]
    part = packed // 2
    row_of = jnp.arange(part)
    pack = (
        (row_of // CAP * ROOM + row_of % CAP)[:, None] == jnp.arange(EXPERTS * ROOM // 2)[None, :]
    ).astype(BF)

    def packing(sent, dy):
        got = list(sent)
        for dz in (2, 1, 3, 0):
            if dz or dy:
                got[dz] = to_expert(sent[dz], dz, dy, 1)
        return dot_f32(pack, jnp.concatenate(got, axis=0), 1, 0).astype(BF)

    own, left, right, partner, far_left, far_right, across = ([] for _ in range(7))
    own = [packing(made[h:EXPERTS:2], h) for h in range(2)]
    for h in range(2):
        left.append(along_x(own[h], 1))
        right.append(along_x(own[h], -1))
        partner.append(pair_y(own[h]))
    for h in range(2):
        far_left.append(along_x(partner[h], 1))
        far_right.append(pair_y(right[h]))
        across.append(along_x(right[h], -1))

    gate_t = gate_weight[0].T
    up_t = up_weight[0].T
    down_t = down_weight[0]
    near = own + left + right + partner
    near_other = [pair_core(v) for v in near]
    near_out = run_group(place, near, near_other, gate_t, up_t, down_t)
    far = far_left + far_right + across
    tied = lax.optimization_barrier((*far, *near_out))
    far = list(tied[: len(far)])
    near_out = tied[len(far) :]
    middle = jnp.concatenate([far[2][third:], far[3][: 2 * third - part]], axis=0)
    last = [along_x(far[0][:third], 1), along_x(middle, -1), pair_y(far[5][2 * third - part :])]
    far = far + last
    far_other = [pair_core(v) for v in far]
    far_out = run_group(place, far, far_other, gate_t, up_t, down_t)

    def add(a, *more):
        total = a.astype(F32)
        for m in more:
            total = total + m.astype(F32)
        return total.astype(BF)

    near_got = pair_core(near_out[1])
    far_got = pair_core(far_out[1])

    def chunk(out, got, i, a=0, b=packed):
        return add(out[0][packed * i + a : packed * i + b], got[packed * i + a : packed * i + b])

    t_last = [chunk(far_out, far_got, 3, third * i, third * (i + 1)) for i in range(3)]
    a_left = along_x(t_last[0], -1)
    a_right = along_x(t_last[1], 1)
    a_pair = pair_y(t_last[2])
    pads = [[(third * i, packed - third * (i + 1)), (0, 0)] for i in range(3)]
    t_far_left = add(chunk(far_out, far_got, 0), jnp.pad(a_left, pads[0]))
    t_far_right = add(chunk(far_out, far_got, 1), jnp.pad(a_right, pads[1]))
    t_across = add(chunk(far_out, far_got, 2), jnp.pad(a_pair, pads[2]))
    b_partner = along_x(t_far_left, -1)
    b_right_pair = pair_y(t_far_right)
    b_right = along_x(t_across, 1)
    hid = gate_t.shape[0]
    rows = (near + far, near_other + far_other)
    sides = [g for t in (2, 3) for g in (near_out[t], far_out[t])]
    gate_grad, up_grad = weight_grads(place, *rows, sides, 0, hid)
    tied = lax.optimization_barrier((b_partner, b_right_pair, b_right, gate_grad, up_grad))
    b_partner, b_right_pair, b_right, gate_grad, up_grad = tied
    c_left = along_x(chunk(near_out, near_got, 1), -1)
    c_right = along_x(add(chunk(near_out, near_got, 2), b_right_pair, b_right), 1)
    c_pair = pair_y(add(chunk(near_out, near_got, 3), b_partner))
    half = tokens.shape[1] // 2
    (down_grad,) = weight_grads(place, *rows, [near_out[4], far_out[4]], half, hid)
    tied = lax.optimization_barrier((c_left, c_right, c_pair, down_grad))
    c_left, c_right, c_pair, down_grad = tied
    home = add(chunk(near_out, near_got, 0), c_left, c_right, c_pair)

    backs = [None] * EXPERTS
    for dy in range(2):
        spread = dot_f32(pack, home[part * dy : part * (dy + 1)], 0, 0).astype(BF)
        for dz in (2, 1, 3, 0):
            k = 2 * dz + dy
            piece = spread[ROOM * dz : ROOM * (dz + 1)]
            if k:
                piece = to_expert(piece, dz, dy, -1)
            backs[k] = piece
    token_grad, route_grad = combine(route_weights, first, second, backs)

    return token_grad, route_grad, gate_grad.T[None], up_grad.T[None], down_grad[None]


def solution(mesh):
    names = ("z", "yh", "yl", "x", "core")
    fine = Mesh(mesh.devices.reshape(4, 2, 2, 4, 2), names)
    ep = names[:4]
    return jax.shard_map(
        per_device,
        mesh=fine,
        in_specs=(
            P(ep, None),
            P(ep, None),
            P(ep, None),
            P(ep, None),
            P(ep, None, "core"),
            P(ep, None, "core"),
            P(ep, "core", None),
        ),
        out_specs=(
            P(ep, "core"),
            P(ep, None),
            P(ep, None, "core"),
            P(ep, None, "core"),
            P(ep, "core", None),
        ),
        check_vma=False,
    )
```

```python
import functools

import jax
import jax.numpy as jnp
from jax import lax
from jax.experimental import pallas as pl
from jax.experimental.pallas import tpu as pltpu
from jax.sharding import Mesh
from jax.sharding import PartitionSpec as P


EXPERTS = 8
TOP = 2
CAP = 12
ROOM = 16
LANES = 128
BF = jnp.bfloat16
F32 = jnp.float32
MIB = 1 << 20


VMEM = pl.BlockSpec(memory_space=pltpu.VMEM)
SMEM = pl.BlockSpec(memory_space=pltpu.SMEM)


def along_x(value, step):
    return lax.ppermute(value, "x", [(i, (i + step) % 4) for i in range(4)])


def pair_y(value):
    return lax.ppermute(value, "yl", [(0, 1), (1, 0)])


def pair_core(value):
    return lax.ppermute(value, "core", [(0, 1), (1, 0)])


def to_expert(value, dz, dy, sign):
    perm = []
    for z in range(4):
        for y in range(4):
            there = (z + sign * dz) % 4 * 4 + (3 - y if dy else y)
            perm.append((z * 4 + y, there))
    return lax.ppermute(value, ("z", "yh", "yl"), perm)


def dot_f32(a, b, left, right):
    return lax.dot_general(a, b, (((left,), (right,)), ((), ())), preferred_element_type=F32)


def slots_kernel(half, place_ref, tok_ref, cot_ref, routes_ref, weights_ref, *refs):
    core, z, yh = place_ref[0], place_ref[1], place_ref[2]
    outs = refs[:EXPERTS]
    first_ref, second_ref, tok_half, cot_half, sems = refs[EXPERTS:]
    here = pl.ds(pl.multiple_of(core * half, half), half)
    loads = [
        pltpu.make_async_copy(tok_ref.at[:, here], tok_half, sems.at[0]),
        pltpu.make_async_copy(cot_ref.at[:, here], cot_half, sems.at[1]),
    ]
    for c in loads:
        c.start()
    rows = tok_half.shape[0]
    routes = routes_ref[...].T
    weights = weights_ref[...].T
    slot = lax.broadcasted_iota(jnp.int32, (rows, EXPERTS * ROOM), 1)
    index = slot // ROOM
    expert = 2 * ((z + index // 2) % 4) + (yh + index % 2) % 2
    is_first = routes[:, 0:1] == expert
    is_second = routes[:, 1:2] == expert
    hot = jnp.where(is_first | is_second, 1.0, 0.0).astype(BF)
    below = lax.broadcasted_iota(jnp.int32, (rows, rows), 1) < lax.broadcasted_iota(
        jnp.int32, (rows, rows), 0
    )
    position = dot_f32(jnp.where(below, 1.0, 0.0).astype(BF), hot, 1, 0)
    fits = position == (slot % ROOM).astype(F32)
    first = jnp.where(is_first & fits, 1.0, 0.0).astype(BF)
    second = jnp.where(is_second & fits, 1.0, 0.0).astype(BF)
    first_ref[...] = first
    second_ref[...] = second
    for c in loads:
        c.wait()
    slot_tok = dot_f32(first + second, tok_half[...], 0, 0).astype(BF)
    cot = cot_half[...].astype(F32)
    scaled = dot_f32(first, (cot * weights[:, 0:1]).astype(BF), 0, 0)
    scaled = scaled + dot_f32(second, (cot * weights[:, 1:2]).astype(BF), 0, 0)
    scaled = scaled.astype(BF)
    for k in range(EXPERTS):
        outs[k][:, :half] = slot_tok[k * ROOM : (k + 1) * ROOM]
        outs[k][:, half:] = scaled[k * ROOM : (k + 1) * ROOM]


def make_slots(place, tokens, cotangent, routes, weights):
    rows, width = tokens.shape
    shapes = [jax.ShapeDtypeStruct((ROOM, width), BF)] * EXPERTS
    shapes += [jax.ShapeDtypeStruct((rows, EXPERTS * ROOM), BF)] * 2
    anywhere = pl.BlockSpec(memory_space=pl.ANY)
    return pl.pallas_call(
        functools.partial(slots_kernel, width // 2),
        out_shape=shapes,
        in_specs=[SMEM, anywhere, anywhere, VMEM, VMEM],
        out_specs=[VMEM] * len(shapes),
        scratch_shapes=[
            pltpu.VMEM((rows, width // 2), BF),
            pltpu.VMEM((rows, width // 2), BF),
            pltpu.SemaphoreType.DMA((2,)),
        ],
        compiler_params=pltpu.CompilerParams(vmem_limit_bytes=60 * MIB),
        cost_estimate=pl.CostEstimate(
            flops=2 * 128 * 24 * width * 2, bytes_accessed=3 * MIB, transcendentals=0
        ),
        name="slots",
    )(place, tokens, cotangent, routes, weights)


def stack_kernel(gate_ref, up_ref, out_ref):
    hid = gate_ref.shape[0]
    wide = out_ref.shape[0] // 2
    for i, ref in enumerate((gate_ref, up_ref)):
        out_ref[wide * i : wide * i + hid] = ref[...]
        out_ref[wide * i + hid : wide * (i + 1)] = jnp.zeros((wide - hid, ref.shape[1]), BF)


def stack_weights(gate, up):
    hid, width = gate.shape
    return pl.pallas_call(
        stack_kernel,
        out_shape=jax.ShapeDtypeStruct((2 * padded(hid), width), BF),
        in_specs=[VMEM] * 2,
        out_specs=VMEM,
        compiler_params=pltpu.CompilerParams(vmem_limit_bytes=16 * MIB),
        cost_estimate=pl.CostEstimate(flops=1000, bytes_accessed=12 * MIB, transcendentals=0),
        name="stack",
    )(gate, up)


def padded(n):
    return -(-n // LANES) * LANES


def group_kernel(count, half, place_ref, *refs):
    core = place_ref[0]
    ours, theirs = refs[:count], refs[count : 2 * count]
    pair_ref, down_ref = refs[2 * count : 2 * count + 2]
    keep_ref, send_ref, sides_out, hidden_out = refs[2 * count + 2 :]
    hid = down_ref.shape[0]
    wide = hidden_out.shape[1]
    here = pl.ds(pl.multiple_of(core * half, half), half)
    there = pl.ds(pl.multiple_of((1 - core) * half, half), half)
    tok = [jnp.concatenate([r[:, :half] for r in side], axis=0) for side in (ours, theirs)]
    pair = dot_f32(tok[0], pair_ref[:, here], 1, 1) + dot_f32(tok[1], pair_ref[:, there], 1, 1)
    cot = [jnp.concatenate([r[:, half:] for r in side], axis=0) for side in (ours, theirs)]
    grad = dot_f32(cot[0], down_ref[:, here], 1, 1) + dot_f32(cot[1], down_ref[:, there], 1, 1)
    gate, up = pair[:, :hid], pair[:, wide : wide + hid]
    sigma = 1.0 / (1.0 + jnp.exp(-gate))
    active = gate * sigma
    hidden = (active * up).astype(BF)
    gate_side = (grad * up * (sigma * (1.0 + gate * (1.0 - sigma)))).astype(BF)
    up_side = (grad * active).astype(BF)
    rest = jnp.zeros((hidden.shape[0], wide - hid), BF)
    hidden_out[:, :hid] = hidden
    hidden_out[:, hid:] = rest
    sides_out[:, :hid] = gate_side
    sides_out[:, hid:wide] = rest
    sides_out[:, wide : wide + hid] = up_side
    sides_out[:, wide + hid :] = rest
    share = jnp.sum(hidden.astype(F32) * grad, axis=1, keepdims=True).astype(BF)
    share = jnp.broadcast_to(share, (share.shape[0], LANES))
    tile = 512
    for base, out in ((core * half, keep_ref), ((1 - core) * half, send_ref)):
        out[:, half:] = share

        @pl.loop(0, half // tile)
        def _(j):
            where = pl.ds(pl.multiple_of(base + j * tile, tile), tile)
            term = dot_f32(sides_out[...], pair_ref[:, where], 1, 0)
            out[:, pl.ds(pl.multiple_of(j * tile, tile), tile)] = term.astype(BF)


def run_group(place, ours, theirs, pair, down):
    rows = sum(r.shape[0] for r in ours)
    hid, width = down.shape
    half = width // 2
    shapes = [jax.ShapeDtypeStruct((rows, half + LANES), BF)] * 2
    shapes += [jax.ShapeDtypeStruct((rows, n * padded(hid)), BF) for n in (2, 1)]
    return pl.pallas_call(
        functools.partial(group_kernel, len(ours), half),
        out_shape=shapes,
        in_specs=[SMEM] + [VMEM] * (2 * len(ours) + 2),
        out_specs=[VMEM] * len(shapes),
        compiler_params=pltpu.CompilerParams(vmem_limit_bytes=40 * MIB),
        cost_estimate=pl.CostEstimate(
            flops=10 * rows * hid * width, bytes_accessed=16 * MIB, transcendentals=rows * hid
        ),
        name="group",
    )(place, *ours, *theirs, pair, down)


def weight_kernel(sizes, offset, half, hid, tile, place_ref, *refs):
    count = len(sizes)
    kinds = len(refs) - 2 * count - 7
    ours, theirs = refs[:count], refs[count : 2 * count]
    sides = refs[2 * count : 2 * count + 2]
    outs = refs[2 * count + 2 : 2 * count + 2 + kinds]
    rows_ref, sides_t, stage, in_sem, out_sem = refs[2 * count + 2 + kinds :]
    core = place_ref[0]
    loads = []
    for s, group in enumerate((ours, theirs)):
        at = 0
        copies = []
        for i, size in enumerate(sizes):
            copies.append(
                pltpu.make_async_copy(
                    group[i].at[:, pl.ds(offset, half)],
                    rows_ref.at[s, pl.ds(at, size), :],
                    in_sem.at[s, i],
                )
            )
            at += size
        loads.append(copies)
    for copies in loads:
        for c in copies:
            c.start()
    depth = sides[0].shape[0]
    wide = sides[0].shape[1] // kinds
    for i in range(2):
        sides_t[:, depth * i : depth * (i + 1)] = sides[i][...].T
    stores = []
    for s in range(2):
        for c in loads[s]:
            c.wait()
        base = (core if s == 0 else 1 - core) * half

        @pl.loop(0, half // tile)
        def _(j):
            to = pl.ds(pl.multiple_of(base + j * tile, tile), tile)
            block = rows_ref[s, :, pl.ds(pl.multiple_of(j * tile, tile), tile)]
            grads = dot_f32(sides_t[...], block, 1, 0).astype(BF)
            for k in range(kinds):
                stage[k, :, to] = grads[wide * k : wide * k + hid]

        whole = pl.ds(pl.multiple_of(base, half), half)
        for k in range(kinds):
            copy = pltpu.make_async_copy(
                stage.at[k, :, whole], outs[k].at[:, whole], out_sem.at[s, k]
            )
            copy.start()
            stores.append(copy)
    for copy in stores:
        copy.wait()


def weight_grads(place, ours, theirs, sides, offset, hid, tile=1024):
    sizes = [r.shape[0] for r in ours]
    rows = sum(sizes)
    width = ours[0].shape[1]
    wide = padded(hid)
    kinds = sides[0].shape[1] // wide
    anywhere = pl.BlockSpec(memory_space=pl.ANY)
    return pl.pallas_call(
        functools.partial(weight_kernel, sizes, offset, width // 2, hid, tile),
        out_shape=[jax.ShapeDtypeStruct((hid, width), BF)] * kinds,
        in_specs=[SMEM] + [anywhere] * (2 * len(sizes)) + [VMEM] * len(sides),
        out_specs=[anywhere] * kinds,
        scratch_shapes=[
            pltpu.VMEM((2, rows, width // 2), BF),
            pltpu.VMEM((kinds * wide, rows), BF),
            pltpu.VMEM((kinds, hid, width), BF),
            pltpu.SemaphoreType.DMA((2, len(sizes))),
            pltpu.SemaphoreType.DMA((2, kinds)),
        ],
        compiler_params=pltpu.CompilerParams(vmem_limit_bytes=28 * MIB),
        cost_estimate=pl.CostEstimate(
            flops=2 * kinds * rows * hid * width, bytes_accessed=14 * MIB, transcendentals=0
        ),
        name="weight_grads",
    )(place, *ours, *theirs, *sides)


def final_kernel(half, weights_ref, first_ref, second_ref, *refs):
    backs = refs[:EXPERTS]
    token_ref, route_ref = refs[EXPERTS:]
    back = jnp.concatenate([b[...] for b in backs], axis=0)
    first, second = first_ref[...], second_ref[...]
    token_ref[...] = dot_f32(first + second, back[:, :half], 1, 0).astype(BF)
    share = back[:, half:]
    route_ref[0:1] = dot_f32(share, first, 0, 1)[0:1] / weights_ref[0:1]
    route_ref[1:2] = dot_f32(share, second, 0, 1)[0:1] / weights_ref[1:2]


def combine(weights, first, second, backs):
    rows = weights.shape[1]
    half = backs[0].shape[1] - LANES
    return pl.pallas_call(
        functools.partial(final_kernel, half),
        out_shape=[
            jax.ShapeDtypeStruct((rows, half), BF),
            jax.ShapeDtypeStruct((TOP, rows), F32),
        ],
        in_specs=[VMEM] * (3 + EXPERTS),
        out_specs=[VMEM] * 2,
        compiler_params=pltpu.CompilerParams(vmem_limit_bytes=8 * MIB),
        cost_estimate=pl.CostEstimate(
            flops=2 * 128 * 24 * half, bytes_accessed=MIB, transcendentals=0
        ),
        name="combine",
    )(weights, first, second, *backs)


def per_device(tokens, cotangent, routes, route_weights, gate_weight, up_weight, down_weight):
    place = jnp.stack([lax.axis_index("core"), lax.axis_index("z"), lax.axis_index("yh")])
    place = place.astype(jnp.int32)
    packed = EXPERTS * CAP
    third = packed // 3

    made = make_slots(place, tokens, cotangent, routes.T, route_weights.T)
    first, second = made[EXPERTS:]
    part = packed // 2
    row_of = jnp.arange(part)
    pack = (
        (row_of // CAP * ROOM + row_of % CAP)[:, None] == jnp.arange(EXPERTS * ROOM // 2)[None, :]
    ).astype(BF)

    def packing(sent, dy):
        got = list(sent)
        for dz in (2, 1, 3, 0):
            if dz or dy:
                got[dz] = to_expert(sent[dz], dz, dy, 1)
        return dot_f32(pack, jnp.concatenate(got, axis=0), 1, 0).astype(BF)

    own, left, right, partner, far_left, far_right, across = ([] for _ in range(7))
    own = [packing(made[h:EXPERTS:2], h) for h in range(2)]
    for h in range(2):
        left.append(along_x(own[h], 1))
        right.append(along_x(own[h], -1))
        partner.append(pair_y(own[h]))
    for h in range(2):
        far_left.append(along_x(partner[h], 1))
        far_right.append(pair_y(right[h]))
        across.append(along_x(right[h], -1))

    down_t = down_weight[0]
    hid = down_t.shape[0]
    pair_t = stack_weights(gate_weight[0].T, up_weight[0].T)
    near = own + left + right + partner
    near_other = [pair_core(v) for v in near]
    near_out = run_group(place, near, near_other, pair_t, down_t)
    far = far_left + far_right + across
    tied = lax.optimization_barrier((*far, *near_out))
    far = list(tied[: len(far)])
    near_out = tied[len(far) :]
    middle = jnp.concatenate([far[2][third:], far[3][: 2 * third - part]], axis=0)
    last = [along_x(far[0][:third], 1), along_x(middle, -1), pair_y(far[5][2 * third - part :])]
    far = far + last
    far_other = [pair_core(v) for v in far]
    far_out = run_group(place, far, far_other, pair_t, down_t)

    def add(a, *more):
        total = a.astype(F32)
        for m in more:
            total = total + m.astype(F32)
        return total.astype(BF)

    near_got = pair_core(near_out[1])
    far_got = pair_core(far_out[1])

    def chunk(out, got, i, a=0, b=packed):
        return add(out[0][packed * i + a : packed * i + b], got[packed * i + a : packed * i + b])

    t_last = [chunk(far_out, far_got, 3, third * i, third * (i + 1)) for i in range(3)]
    a_left = along_x(t_last[0], -1)
    a_right = along_x(t_last[1], 1)
    a_pair = pair_y(t_last[2])
    pads = [[(third * i, packed - third * (i + 1)), (0, 0)] for i in range(3)]
    t_far_left = add(chunk(far_out, far_got, 0), jnp.pad(a_left, pads[0]))
    t_far_right = add(chunk(far_out, far_got, 1), jnp.pad(a_right, pads[1]))
    t_across = add(chunk(far_out, far_got, 2), jnp.pad(a_pair, pads[2]))
    b_partner = along_x(t_far_left, -1)
    b_right_pair = pair_y(t_far_right)
    b_right = along_x(t_across, 1)
    rows = (near + far, near_other + far_other)
    sides = [near_out[2], far_out[2]]
    gate_grad, up_grad = weight_grads(place, *rows, sides, 0, hid)
    tied = lax.optimization_barrier((b_partner, b_right_pair, b_right, gate_grad, up_grad))
    b_partner, b_right_pair, b_right, gate_grad, up_grad = tied
    c_left = along_x(chunk(near_out, near_got, 1), -1)
    c_right = along_x(add(chunk(near_out, near_got, 2), b_right_pair, b_right), 1)
    c_pair = pair_y(add(chunk(near_out, near_got, 3), b_partner))
    half = tokens.shape[1] // 2
    (down_grad,) = weight_grads(place, *rows, [near_out[3], far_out[3]], half, hid)
    tied = lax.optimization_barrier((c_left, c_right, c_pair, down_grad))
    c_left, c_right, c_pair, down_grad = tied
    home = add(chunk(near_out, near_got, 0), c_left, c_right, c_pair)

    backs = [None] * EXPERTS
    for dy in range(2):
        spread = dot_f32(pack, home[part * dy : part * (dy + 1)], 0, 0).astype(BF)
        for dz in (2, 1, 3, 0):
            k = 2 * dz + dy
            piece = spread[ROOM * dz : ROOM * (dz + 1)]
            if k:
                piece = to_expert(piece, dz, dy, -1)
            backs[k] = piece
    token_grad, route_grad = combine(route_weights.T, first, second, backs)

    return token_grad, route_grad.T, gate_grad.T[None], up_grad.T[None], down_grad[None]


def solution(mesh):
    names = ("z", "yh", "yl", "x", "core")
    fine = Mesh(mesh.devices.reshape(4, 2, 2, 4, 2), names)
    ep = names[:4]
    return jax.shard_map(
        per_device,
        mesh=fine,
        in_specs=(
            P(ep, None),
            P(ep, None),
            P(ep, None),
            P(ep, None),
            P(ep, None, "core"),
            P(ep, None, "core"),
            P(ep, "core", None),
        ),
        out_specs=(
            P(ep, "core"),
            P(ep, None),
            P(ep, None, "core"),
            P(ep, None, "core"),
            P(ep, "core", None),
        ),
        check_vma=False,
    )
```

```python
import functools

import jax
import jax.numpy as jnp
from jax import lax
from jax.experimental import pallas as pl
from jax.experimental.pallas import tpu as pltpu
from jax.sharding import Mesh
from jax.sharding import PartitionSpec as P


EXPERTS = 8
TOP = 2
CAP = 12
ROOM = 16
LANES = 128
BF = jnp.bfloat16
F32 = jnp.float32
MIB = 1 << 20


VMEM = pl.BlockSpec(memory_space=pltpu.VMEM)
SMEM = pl.BlockSpec(memory_space=pltpu.SMEM)


def along_x(value, step):
    return lax.ppermute(value, "x", [(i, (i + step) % 4) for i in range(4)])


def pair_y(value):
    return lax.ppermute(value, "yl", [(0, 1), (1, 0)])


def pair_core(value):
    return lax.ppermute(value, "core", [(0, 1), (1, 0)])


def to_expert(value, dz, dy, sign):
    perm = []
    for z in range(4):
        for y in range(4):
            there = (z + sign * dz) % 4 * 4 + (3 - y if dy else y)
            perm.append((z * 4 + y, there))
    return lax.ppermute(value, ("z", "yh", "yl"), perm)


def dot_f32(a, b, left, right):
    return lax.dot_general(a, b, (((left,), (right,)), ((), ())), preferred_element_type=F32)


def slots_kernel(half, place_ref, tok_ref, cot_ref, routes_ref, weights_ref, *refs):
    core, z, yh = place_ref[0], place_ref[1], place_ref[2]
    outs = refs[:EXPERTS]
    first_ref, second_ref, tok_half, cot_half, sems = refs[EXPERTS:]
    here = pl.ds(pl.multiple_of(core * half, half), half)
    loads = [
        pltpu.make_async_copy(tok_ref.at[:, here], tok_half, sems.at[0]),
        pltpu.make_async_copy(cot_ref.at[:, here], cot_half, sems.at[1]),
    ]
    for c in loads:
        c.start()
    rows = tok_half.shape[0]
    routes = routes_ref[...].T
    weights = weights_ref[...].T
    slot = lax.broadcasted_iota(jnp.int32, (rows, EXPERTS * ROOM), 1)
    index = slot // ROOM
    expert = 2 * ((z + index // 2) % 4) + (yh + index % 2) % 2
    is_first = routes[:, 0:1] == expert
    is_second = routes[:, 1:2] == expert
    hot = jnp.where(is_first | is_second, 1.0, 0.0).astype(BF)
    below = lax.broadcasted_iota(jnp.int32, (rows, rows), 1) < lax.broadcasted_iota(
        jnp.int32, (rows, rows), 0
    )
    position = dot_f32(jnp.where(below, 1.0, 0.0).astype(BF), hot, 1, 0)
    fits = position == (slot % ROOM).astype(F32)
    first = jnp.where(is_first & fits, 1.0, 0.0).astype(BF)
    second = jnp.where(is_second & fits, 1.0, 0.0).astype(BF)
    first_ref[...] = first
    second_ref[...] = second
    for c in loads:
        c.wait()
    slot_tok = dot_f32(first + second, tok_half[...], 0, 0).astype(BF)
    cot = cot_half[...].astype(F32)
    scaled = dot_f32(first, (cot * weights[:, 0:1]).astype(BF), 0, 0)
    scaled = scaled + dot_f32(second, (cot * weights[:, 1:2]).astype(BF), 0, 0)
    scaled = scaled.astype(BF)
    for k in range(EXPERTS):
        outs[k][:, :half] = slot_tok[k * ROOM : (k + 1) * ROOM]
        outs[k][:, half:] = scaled[k * ROOM : (k + 1) * ROOM]


def make_slots(place, tokens, cotangent, routes, weights):
    rows, width = tokens.shape
    shapes = [jax.ShapeDtypeStruct((ROOM, width), BF)] * EXPERTS
    shapes += [jax.ShapeDtypeStruct((rows, EXPERTS * ROOM), BF)] * 2
    anywhere = pl.BlockSpec(memory_space=pl.ANY)
    return pl.pallas_call(
        functools.partial(slots_kernel, width // 2),
        out_shape=shapes,
        in_specs=[SMEM, anywhere, anywhere, VMEM, VMEM],
        out_specs=[VMEM] * len(shapes),
        scratch_shapes=[
            pltpu.VMEM((rows, width // 2), BF),
            pltpu.VMEM((rows, width // 2), BF),
            pltpu.SemaphoreType.DMA((2,)),
        ],
        compiler_params=pltpu.CompilerParams(vmem_limit_bytes=60 * MIB),
        cost_estimate=pl.CostEstimate(
            flops=2 * 128 * 24 * width * 2, bytes_accessed=3 * MIB, transcendentals=0
        ),
        name="slots",
    )(place, tokens, cotangent, routes, weights)


def stack_kernel(gate_ref, up_ref, out_ref):
    hid = gate_ref.shape[0]
    wide = out_ref.shape[0] // 2
    for i, ref in enumerate((gate_ref, up_ref)):
        out_ref[wide * i : wide * i + hid] = ref[...]
        out_ref[wide * i + hid : wide * (i + 1)] = jnp.zeros((wide - hid, ref.shape[1]), BF)


def stack_weights(gate, up):
    hid, width = gate.shape
    return pl.pallas_call(
        stack_kernel,
        out_shape=jax.ShapeDtypeStruct((2 * padded(hid), width), BF),
        in_specs=[VMEM] * 2,
        out_specs=VMEM,
        compiler_params=pltpu.CompilerParams(vmem_limit_bytes=16 * MIB),
        cost_estimate=pl.CostEstimate(flops=1000, bytes_accessed=12 * MIB, transcendentals=0),
        name="stack",
    )(gate, up)


def padded(n):
    return -(-n // LANES) * LANES


def group_kernel(count, half, place_ref, *refs):
    core = place_ref[0]
    ours, theirs = refs[:count], refs[count : 2 * count]
    pair_ref, down_ref = refs[2 * count : 2 * count + 2]
    send_ref, share_out, sides_out, hidden_out = refs[2 * count + 2 :]
    hid = down_ref.shape[0]
    wide = hidden_out.shape[1]
    here = pl.ds(pl.multiple_of(core * half, half), half)
    there = pl.ds(pl.multiple_of((1 - core) * half, half), half)
    tok = [jnp.concatenate([r[:, :half] for r in side], axis=0) for side in (ours, theirs)]
    pair = dot_f32(tok[0], pair_ref[:, here], 1, 1) + dot_f32(tok[1], pair_ref[:, there], 1, 1)
    cot = [jnp.concatenate([r[:, half:] for r in side], axis=0) for side in (ours, theirs)]
    grad = dot_f32(cot[0], down_ref[:, here], 1, 1) + dot_f32(cot[1], down_ref[:, there], 1, 1)
    gate, up = pair[:, :hid], pair[:, wide : wide + hid]
    sigma = 1.0 / (1.0 + jnp.exp(-gate))
    active = gate * sigma
    hidden = (active * up).astype(BF)
    gate_side = (grad * up * (sigma * (1.0 + gate * (1.0 - sigma)))).astype(BF)
    up_side = (grad * active).astype(BF)
    rest = jnp.zeros((hidden.shape[0], wide - hid), BF)
    hidden_out[:, :hid] = hidden
    hidden_out[:, hid:] = rest
    sides_out[:, :hid] = gate_side
    sides_out[:, hid:wide] = rest
    sides_out[:, wide : wide + hid] = up_side
    sides_out[:, wide + hid :] = rest
    share = jnp.sum(hidden.astype(F32) * grad, axis=1, keepdims=True).astype(BF)
    share = jnp.broadcast_to(share, (share.shape[0], LANES))
    share_out[...] = share
    token_terms(sides_out, pair_ref, share, (1 - core) * half, send_ref)


def token_terms(sides_ref, pair_ref, share, base, out):
    half = out.shape[1] - LANES
    tile = 1024
    out[:, half:] = share

    @pl.loop(0, half // tile)
    def _(j):
        where = pl.ds(pl.multiple_of(base + j * tile, tile), tile)
        term = dot_f32(sides_ref[...], pair_ref[:, where], 1, 0)
        out[:, pl.ds(pl.multiple_of(j * tile, tile), tile)] = term.astype(BF)


def keep_kernel(half, place_ref, sides_ref, share_ref, pair_ref, out_ref):
    token_terms(sides_ref, pair_ref, share_ref[...], place_ref[0] * half, out_ref)


def keep_half(place, sides, share, pair):
    rows = sides.shape[0]
    half = pair.shape[1] // 2
    return pl.pallas_call(
        functools.partial(keep_kernel, half),
        out_shape=jax.ShapeDtypeStruct((rows, half + LANES), BF),
        in_specs=[SMEM] + [VMEM] * 3,
        out_specs=VMEM,
        compiler_params=pltpu.CompilerParams(vmem_limit_bytes=12 * MIB),
        cost_estimate=pl.CostEstimate(
            flops=2 * rows * pair.shape[0] * half, bytes_accessed=8 * MIB, transcendentals=0
        ),
        name="keep",
    )(place, sides, share, pair)


def run_group(place, ours, theirs, pair, down):
    rows = sum(r.shape[0] for r in ours)
    hid, width = down.shape
    half = width // 2
    lanes = (half + LANES, LANES, 2 * padded(hid), padded(hid))
    shapes = [jax.ShapeDtypeStruct((rows, n), BF) for n in lanes]
    return pl.pallas_call(
        functools.partial(group_kernel, len(ours), half),
        out_shape=shapes,
        in_specs=[SMEM] + [VMEM] * (2 * len(ours) + 2),
        out_specs=[VMEM] * len(shapes),
        compiler_params=pltpu.CompilerParams(vmem_limit_bytes=20 * MIB),
        cost_estimate=pl.CostEstimate(
            flops=8 * rows * hid * width, bytes_accessed=16 * MIB, transcendentals=rows * hid
        ),
        name="group",
    )(place, *ours, *theirs, pair, down)


def weight_kernel(sizes, offset, half, hid, tile, place_ref, *refs):
    count = len(sizes)
    kinds = len(refs) - 2 * count - 7
    ours, theirs = refs[:count], refs[count : 2 * count]
    sides = refs[2 * count : 2 * count + 2]
    outs = refs[2 * count + 2 : 2 * count + 2 + kinds]
    rows_ref, sides_t, stage, in_sem, out_sem = refs[2 * count + 2 + kinds :]
    core = place_ref[0]
    loads = []
    for s, group in enumerate((ours, theirs)):
        at = 0
        copies = []
        for i, size in enumerate(sizes):
            copies.append(
                pltpu.make_async_copy(
                    group[i].at[:, pl.ds(offset, half)],
                    rows_ref.at[s, pl.ds(at, size), :],
                    in_sem.at[s, i],
                )
            )
            at += size
        loads.append(copies)
    for copies in loads:
        for c in copies:
            c.start()
    depth = sides[0].shape[0]
    wide = sides[0].shape[1] // kinds
    for i in range(2):
        sides_t[:, depth * i : depth * (i + 1)] = sides[i][...].T
    stores = []
    for s in range(2):
        for c in loads[s]:
            c.wait()
        base = (core if s == 0 else 1 - core) * half

        @pl.loop(0, half // tile)
        def _(j):
            to = pl.ds(pl.multiple_of(base + j * tile, tile), tile)
            block = rows_ref[s, :, pl.ds(pl.multiple_of(j * tile, tile), tile)]
            grads = dot_f32(sides_t[...], block, 1, 0).astype(BF)
            for k in range(kinds):
                stage[k, :, to] = grads[wide * k : wide * k + hid]

        whole = pl.ds(pl.multiple_of(base, half), half)
        for k in range(kinds):
            copy = pltpu.make_async_copy(
                stage.at[k, :, whole], outs[k].at[:, whole], out_sem.at[s, k]
            )
            copy.start()
            stores.append(copy)
    for copy in stores:
        copy.wait()


def weight_grads(place, ours, theirs, sides, offset, hid, tile=1024):
    sizes = [r.shape[0] for r in ours]
    rows = sum(sizes)
    width = ours[0].shape[1]
    wide = padded(hid)
    kinds = sides[0].shape[1] // wide
    anywhere = pl.BlockSpec(memory_space=pl.ANY)
    return pl.pallas_call(
        functools.partial(weight_kernel, sizes, offset, width // 2, hid, tile),
        out_shape=[jax.ShapeDtypeStruct((hid, width), BF)] * kinds,
        in_specs=[SMEM] + [anywhere] * (2 * len(sizes)) + [VMEM] * len(sides),
        out_specs=[anywhere] * kinds,
        scratch_shapes=[
            pltpu.VMEM((2, rows, width // 2), BF),
            pltpu.VMEM((kinds * wide, rows), BF),
            pltpu.VMEM((kinds, hid, width), BF),
            pltpu.SemaphoreType.DMA((2, len(sizes))),
            pltpu.SemaphoreType.DMA((2, kinds)),
        ],
        compiler_params=pltpu.CompilerParams(vmem_limit_bytes=22 * MIB),
        cost_estimate=pl.CostEstimate(
            flops=2 * kinds * rows * hid * width, bytes_accessed=14 * MIB, transcendentals=0
        ),
        name="weight_grads",
    )(place, *ours, *theirs, *sides)


def final_kernel(half, weights_ref, first_ref, second_ref, *refs):
    backs = refs[:EXPERTS]
    token_ref, route_ref = refs[EXPERTS:]
    back = jnp.concatenate([b[...] for b in backs], axis=0)
    first, second = first_ref[...], second_ref[...]
    token_ref[...] = dot_f32(first + second, back[:, :half], 1, 0).astype(BF)
    share = back[:, half:]
    route_ref[0:1] = dot_f32(share, first, 0, 1)[0:1] / weights_ref[0:1]
    route_ref[1:2] = dot_f32(share, second, 0, 1)[0:1] / weights_ref[1:2]


def combine(weights, first, second, backs):
    rows = weights.shape[1]
    half = backs[0].shape[1] - LANES
    return pl.pallas_call(
        functools.partial(final_kernel, half),
        out_shape=[
            jax.ShapeDtypeStruct((rows, half), BF),
            jax.ShapeDtypeStruct((TOP, rows), F32),
        ],
        in_specs=[VMEM] * (3 + EXPERTS),
        out_specs=[VMEM] * 2,
        compiler_params=pltpu.CompilerParams(vmem_limit_bytes=8 * MIB),
        cost_estimate=pl.CostEstimate(
            flops=2 * 128 * 24 * half, bytes_accessed=MIB, transcendentals=0
        ),
        name="combine",
    )(weights, first, second, *backs)


def per_device(tokens, cotangent, routes, route_weights, gate_weight, up_weight, down_weight):
    place = jnp.stack([lax.axis_index("core"), lax.axis_index("z"), lax.axis_index("yh")])
    place = place.astype(jnp.int32)
    packed = EXPERTS * CAP
    third = packed // 3

    made = make_slots(place, tokens, cotangent, routes.T, route_weights.T)
    first, second = made[EXPERTS:]
    part = packed // 2
    row_of = jnp.arange(part)
    pack = (
        (row_of // CAP * ROOM + row_of % CAP)[:, None] == jnp.arange(EXPERTS * ROOM // 2)[None, :]
    ).astype(BF)

    def packing(sent, dy):
        got = list(sent)
        for dz in (2, 1, 3, 0):
            if dz or dy:
                got[dz] = to_expert(sent[dz], dz, dy, 1)
        return dot_f32(pack, jnp.concatenate(got, axis=0), 1, 0).astype(BF)

    own, left, right, partner, far_left, far_right, across = ([] for _ in range(7))
    own = [packing(made[h:EXPERTS:2], h) for h in range(2)]
    for h in range(2):
        left.append(along_x(own[h], 1))
        right.append(along_x(own[h], -1))
        partner.append(pair_y(own[h]))
    for h in range(2):
        far_left.append(along_x(partner[h], 1))
        far_right.append(pair_y(right[h]))
        across.append(along_x(right[h], -1))

    down_t = down_weight[0]
    hid = down_t.shape[0]
    pair_t = stack_weights(gate_weight[0].T, up_weight[0].T)
    near = own + left + right + partner
    near_other = [pair_core(v) for v in near]
    near_out = run_group(place, near, near_other, pair_t, down_t)
    far = far_left + far_right + across
    tied = lax.optimization_barrier((*far, *near_out))
    far = list(tied[: len(far)])
    near_out = tied[len(far) :]
    middle = jnp.concatenate([far[2][third:], far[3][: 2 * third - part]], axis=0)
    last = [along_x(far[0][:third], 1), along_x(middle, -1), pair_y(far[5][2 * third - part :])]
    far = far + last
    far_other = [pair_core(v) for v in far]
    far_out = run_group(place, far, far_other, pair_t, down_t)

    def add(a, *more):
        total = a.astype(F32)
        for m in more:
            total = total + m.astype(F32)
        return total.astype(BF)

    far_got = pair_core(far_out[0])
    near_got = pair_core(near_out[0])
    far_keep = keep_half(place, far_out[2], far_out[1], pair_t)
    near_keep = keep_half(place, near_out[2], near_out[1], pair_t)

    def chunk(keep, got, i, a=0, b=packed):
        return add(keep[packed * i + a : packed * i + b], got[packed * i + a : packed * i + b])

    t_last = [chunk(far_keep, far_got, 3, third * i, third * (i + 1)) for i in range(3)]
    a_left = along_x(t_last[0], -1)
    a_right = along_x(t_last[1], 1)
    a_pair = pair_y(t_last[2])
    pads = [[(third * i, packed - third * (i + 1)), (0, 0)] for i in range(3)]
    t_far_left = add(chunk(far_keep, far_got, 0), jnp.pad(a_left, pads[0]))
    t_far_right = add(chunk(far_keep, far_got, 1), jnp.pad(a_right, pads[1]))
    t_across = add(chunk(far_keep, far_got, 2), jnp.pad(a_pair, pads[2]))
    b_partner = along_x(t_far_left, -1)
    b_right_pair = pair_y(t_far_right)
    b_right = along_x(t_across, 1)
    rows = (near + far, near_other + far_other)
    sides = [near_out[2], far_out[2]]
    gate_grad, up_grad = weight_grads(place, *rows, sides, 0, hid)
    tied = lax.optimization_barrier((b_partner, b_right_pair, b_right, gate_grad, up_grad))
    b_partner, b_right_pair, b_right, gate_grad, up_grad = tied
    c_left = along_x(chunk(near_keep, near_got, 1), -1)
    c_right = along_x(add(chunk(near_keep, near_got, 2), b_right_pair, b_right), 1)
    c_pair = pair_y(add(chunk(near_keep, near_got, 3), b_partner))
    half = tokens.shape[1] // 2
    (down_grad,) = weight_grads(place, *rows, [near_out[3], far_out[3]], half, hid)
    tied = lax.optimization_barrier((c_left, c_right, c_pair, down_grad))
    c_left, c_right, c_pair, down_grad = tied
    home = add(chunk(near_keep, near_got, 0), c_left, c_right, c_pair)

    backs = [None] * EXPERTS
    for dy in range(2):
        spread = dot_f32(pack, home[part * dy : part * (dy + 1)], 0, 0).astype(BF)
        for dz in (2, 1, 3, 0):
            k = 2 * dz + dy
            piece = spread[ROOM * dz : ROOM * (dz + 1)]
            if k:
                piece = to_expert(piece, dz, dy, -1)
            backs[k] = piece
    token_grad, route_grad = combine(route_weights.T, first, second, backs)

    return token_grad, route_grad.T, gate_grad.T[None], up_grad.T[None], down_grad[None]


def solution(mesh):
    names = ("z", "yh", "yl", "x", "core")
    fine = Mesh(mesh.devices.reshape(4, 2, 2, 4, 2), names)
    ep = names[:4]
    return jax.shard_map(
        per_device,
        mesh=fine,
        in_specs=(
            P(ep, None),
            P(ep, None),
            P(ep, None),
            P(ep, None),
            P(ep, None, "core"),
            P(ep, None, "core"),
            P(ep, "core", None),
        ),
        out_specs=(
            P(ep, "core"),
            P(ep, None),
            P(ep, None, "core"),
            P(ep, None, "core"),
            P(ep, "core", None),
        ),
        check_vma=False,
    )
```

```python
import functools

import jax
import jax.numpy as jnp
from jax import lax
from jax.experimental import pallas as pl
from jax.experimental.pallas import tpu as pltpu
from jax.sharding import Mesh
from jax.sharding import PartitionSpec as P


EXPERTS = 8
TOP = 2
CAP = 12
ROOM = 16
LANES = 128
BF = jnp.bfloat16
F32 = jnp.float32
MIB = 1 << 20


VMEM = pl.BlockSpec(memory_space=pltpu.VMEM)
SMEM = pl.BlockSpec(memory_space=pltpu.SMEM)


def along_x(value, step):
    return lax.ppermute(value, "x", [(i, (i + step) % 4) for i in range(4)])


def pair_y(value):
    return lax.ppermute(value, "yl", [(0, 1), (1, 0)])


def pair_core(value):
    return lax.ppermute(value, "core", [(0, 1), (1, 0)])


def to_expert(value, dz, dy, sign):
    perm = []
    for z in range(4):
        for y in range(4):
            there = (z + sign * dz) % 4 * 4 + (3 - y if dy else y)
            perm.append((z * 4 + y, there))
    return lax.ppermute(value, ("z", "yh", "yl"), perm)


def dot_f32(a, b, left, right):
    return lax.dot_general(a, b, (((left,), (right,)), ((), ())), preferred_element_type=F32)


def slots_kernel(half, place_ref, tok_ref, cot_ref, routes_ref, weights_ref, *refs):
    core, z, yh = place_ref[0], place_ref[1], place_ref[2]
    outs = refs[:EXPERTS]
    first_ref, second_ref, tok_half, cot_half, sems = refs[EXPERTS:]
    here = pl.ds(pl.multiple_of(core * half, half), half)
    loads = [
        pltpu.make_async_copy(tok_ref.at[:, here], tok_half, sems.at[0]),
        pltpu.make_async_copy(cot_ref.at[:, here], cot_half, sems.at[1]),
    ]
    for c in loads:
        c.start()
    rows = tok_half.shape[0]
    routes = routes_ref[...].T
    weights = weights_ref[...].T
    slot = lax.broadcasted_iota(jnp.int32, (rows, EXPERTS * ROOM), 1)
    index = slot // ROOM
    expert = 2 * ((z + index // 2) % 4) + (yh + index % 2) % 2
    is_first = routes[:, 0:1] == expert
    is_second = routes[:, 1:2] == expert
    hot = jnp.where(is_first | is_second, 1.0, 0.0).astype(BF)
    below = lax.broadcasted_iota(jnp.int32, (rows, rows), 1) < lax.broadcasted_iota(
        jnp.int32, (rows, rows), 0
    )
    position = dot_f32(jnp.where(below, 1.0, 0.0).astype(BF), hot, 1, 0)
    fits = position == (slot % ROOM).astype(F32)
    first = jnp.where(is_first & fits, 1.0, 0.0).astype(BF)
    second = jnp.where(is_second & fits, 1.0, 0.0).astype(BF)
    first_ref[...] = first
    second_ref[...] = second
    for c in loads:
        c.wait()
    slot_tok = dot_f32(first + second, tok_half[...], 0, 0).astype(BF)
    cot = cot_half[...].astype(F32)
    scaled = dot_f32(first, (cot * weights[:, 0:1]).astype(BF), 0, 0)
    scaled = scaled + dot_f32(second, (cot * weights[:, 1:2]).astype(BF), 0, 0)
    scaled = scaled.astype(BF)
    for k in range(EXPERTS):
        outs[k][:, :half] = slot_tok[k * ROOM : (k + 1) * ROOM]
        outs[k][:, half:] = scaled[k * ROOM : (k + 1) * ROOM]


def make_slots(place, tokens, cotangent, routes, weights):
    rows, width = tokens.shape
    shapes = [jax.ShapeDtypeStruct((ROOM, width), BF)] * EXPERTS
    shapes += [jax.ShapeDtypeStruct((rows, EXPERTS * ROOM), BF)] * 2
    anywhere = pl.BlockSpec(memory_space=pl.ANY)
    return pl.pallas_call(
        functools.partial(slots_kernel, width // 2),
        out_shape=shapes,
        in_specs=[SMEM, anywhere, anywhere, VMEM, VMEM],
        out_specs=[VMEM] * len(shapes),
        scratch_shapes=[
            pltpu.VMEM((rows, width // 2), BF),
            pltpu.VMEM((rows, width // 2), BF),
            pltpu.SemaphoreType.DMA((2,)),
        ],
        compiler_params=pltpu.CompilerParams(vmem_limit_bytes=60 * MIB),
        cost_estimate=pl.CostEstimate(
            flops=2 * 128 * 24 * width * 2, bytes_accessed=3 * MIB, transcendentals=0
        ),
        name="slots",
    )(place, tokens, cotangent, routes, weights)


def stack_kernel(gate_ref, up_ref, out_ref):
    hid = gate_ref.shape[0]
    wide = out_ref.shape[0] // 2
    for i, ref in enumerate((gate_ref, up_ref)):
        out_ref[wide * i : wide * i + hid] = ref[...]
        out_ref[wide * i + hid : wide * (i + 1)] = jnp.zeros((wide - hid, ref.shape[1]), BF)


def stack_weights(gate, up):
    hid, width = gate.shape
    return pl.pallas_call(
        stack_kernel,
        out_shape=jax.ShapeDtypeStruct((2 * padded(hid), width), BF),
        in_specs=[VMEM] * 2,
        out_specs=VMEM,
        compiler_params=pltpu.CompilerParams(vmem_limit_bytes=16 * MIB),
        cost_estimate=pl.CostEstimate(flops=1000, bytes_accessed=12 * MIB, transcendentals=0),
        name="stack",
    )(gate, up)


def padded(n):
    return -(-n // LANES) * LANES


def group_kernel(count, half, place_ref, *refs):
    core = place_ref[0]
    ours, theirs = refs[:count], refs[count : 2 * count]
    pair_ref, down_ref = refs[2 * count : 2 * count + 2]
    send_ref, share_out, sides_out, hidden_out = refs[2 * count + 2 :]
    hid = down_ref.shape[0]
    wide = hidden_out.shape[1]
    here = pl.ds(pl.multiple_of(core * half, half), half)
    there = pl.ds(pl.multiple_of((1 - core) * half, half), half)
    tok = [jnp.concatenate([r[:, :half] for r in side], axis=0) for side in (ours, theirs)]
    pair = dot_f32(tok[0], pair_ref[:, here], 1, 1) + dot_f32(tok[1], pair_ref[:, there], 1, 1)
    cot = [jnp.concatenate([r[:, half:] for r in side], axis=0) for side in (ours, theirs)]
    grad = dot_f32(cot[0], down_ref[:, here], 1, 1) + dot_f32(cot[1], down_ref[:, there], 1, 1)
    gate, up = pair[:, :hid], pair[:, wide : wide + hid]
    sigma = 1.0 / (1.0 + jnp.exp(-gate))
    active = gate * sigma
    hidden = (active * up).astype(BF)
    gate_side = (grad * up * (sigma * (1.0 + gate * (1.0 - sigma)))).astype(BF)
    up_side = (grad * active).astype(BF)
    rest = jnp.zeros((hidden.shape[0], wide - hid), BF)
    hidden_out[:, :hid] = hidden
    hidden_out[:, hid:] = rest
    sides_out[:, :hid] = gate_side
    sides_out[:, hid:wide] = rest
    sides_out[:, wide : wide + hid] = up_side
    sides_out[:, wide + hid :] = rest
    share = jnp.sum(hidden.astype(F32) * grad, axis=1, keepdims=True).astype(BF)
    share = jnp.broadcast_to(share, (share.shape[0], LANES))
    share_out[...] = share
    token_terms(sides_out, pair_ref, share, (1 - core) * half, send_ref)


def token_terms(sides_ref, pair_ref, share, base, out):
    half = out.shape[1] - LANES
    tile = 1024
    out[:, half:] = share

    @pl.loop(0, half // tile)
    def _(j):
        where = pl.ds(pl.multiple_of(base + j * tile, tile), tile)
        term = dot_f32(sides_ref[...], pair_ref[:, where], 1, 0)
        out[:, pl.ds(pl.multiple_of(j * tile, tile), tile)] = term.astype(BF)


def keep_kernel(half, place_ref, sides_ref, share_ref, pair_ref, out_ref):
    token_terms(sides_ref, pair_ref, share_ref[...], place_ref[0] * half, out_ref)


def keep_half(place, sides, share, pair):
    rows = sides.shape[0]
    half = pair.shape[1] // 2
    return pl.pallas_call(
        functools.partial(keep_kernel, half),
        out_shape=jax.ShapeDtypeStruct((rows, half + LANES), BF),
        in_specs=[SMEM] + [VMEM] * 3,
        out_specs=VMEM,
        compiler_params=pltpu.CompilerParams(vmem_limit_bytes=12 * MIB),
        cost_estimate=pl.CostEstimate(
            flops=2 * rows * pair.shape[0] * half, bytes_accessed=8 * MIB, transcendentals=0
        ),
        name="keep",
    )(place, sides, share, pair)


def run_group(place, ours, theirs, pair, down):
    rows = sum(r.shape[0] for r in ours)
    hid, width = down.shape
    half = width // 2
    lanes = (half + LANES, LANES, 2 * padded(hid), padded(hid))
    shapes = [jax.ShapeDtypeStruct((rows, n), BF) for n in lanes]
    return pl.pallas_call(
        functools.partial(group_kernel, len(ours), half),
        out_shape=shapes,
        in_specs=[SMEM] + [VMEM] * (2 * len(ours) + 2),
        out_specs=[VMEM] * len(shapes),
        compiler_params=pltpu.CompilerParams(vmem_limit_bytes=20 * MIB),
        cost_estimate=pl.CostEstimate(
            flops=8 * rows * hid * width, bytes_accessed=16 * MIB, transcendentals=rows * hid
        ),
        name="group",
    )(place, *ours, *theirs, pair, down)


def weight_kernel(sizes, offset, half, hid, tile, place_ref, *refs):
    count = len(sizes)
    kinds = len(refs) - 2 * count - 7
    ours, theirs = refs[:count], refs[count : 2 * count]
    sides = refs[2 * count : 2 * count + 2]
    outs = refs[2 * count + 2 : 2 * count + 2 + kinds]
    rows_ref, sides_t, stage, in_sem, out_sem = refs[2 * count + 2 + kinds :]
    core = place_ref[0]
    loads = []
    for s, group in enumerate((ours, theirs)):
        at = 0
        copies = []
        for i, size in enumerate(sizes):
            copies.append(
                pltpu.make_async_copy(
                    group[i].at[:, pl.ds(offset, half)],
                    rows_ref.at[s, pl.ds(at, size), :],
                    in_sem.at[s, i],
                )
            )
            at += size
        loads.append(copies)
    for copies in loads:
        for c in copies:
            c.start()
    depth = sides[0].shape[0]
    wide = sides[0].shape[1] // kinds
    for i in range(2):
        sides_t[:, depth * i : depth * (i + 1)] = sides[i][...].T
    stores = []
    for s in range(2):
        for c in loads[s]:
            c.wait()
        base = (core if s == 0 else 1 - core) * half

        @pl.loop(0, half // tile)
        def _(j):
            to = pl.ds(pl.multiple_of(base + j * tile, tile), tile)
            block = rows_ref[s, :, pl.ds(pl.multiple_of(j * tile, tile), tile)]
            grads = dot_f32(sides_t[...], block, 1, 0).astype(BF)
            for k in range(kinds):
                stage[k, :, to] = grads[wide * k : wide * k + hid]

        whole = pl.ds(pl.multiple_of(base, half), half)
        for k in range(kinds):
            copy = pltpu.make_async_copy(
                stage.at[k, :, whole], outs[k].at[:, whole], out_sem.at[s, k]
            )
            copy.start()
            stores.append(copy)
    for copy in stores:
        copy.wait()


def weight_grads(place, ours, theirs, sides, offset, hid, tile=1024):
    sizes = [r.shape[0] for r in ours]
    rows = sum(sizes)
    width = ours[0].shape[1]
    wide = padded(hid)
    kinds = sides[0].shape[1] // wide
    anywhere = pl.BlockSpec(memory_space=pl.ANY)
    return pl.pallas_call(
        functools.partial(weight_kernel, sizes, offset, width // 2, hid, tile),
        out_shape=[jax.ShapeDtypeStruct((hid, width), BF)] * kinds,
        in_specs=[SMEM] + [anywhere] * (2 * len(sizes)) + [VMEM] * len(sides),
        out_specs=[anywhere] * kinds,
        scratch_shapes=[
            pltpu.VMEM((2, rows, width // 2), BF),
            pltpu.VMEM((kinds * wide, rows), BF),
            pltpu.VMEM((kinds, hid, width), BF),
            pltpu.SemaphoreType.DMA((2, len(sizes))),
            pltpu.SemaphoreType.DMA((2, kinds)),
        ],
        compiler_params=pltpu.CompilerParams(vmem_limit_bytes=22 * MIB),
        cost_estimate=pl.CostEstimate(
            flops=2 * kinds * rows * hid * width, bytes_accessed=14 * MIB, transcendentals=0
        ),
        name="weight_grads",
    )(place, *ours, *theirs, *sides)


def final_kernel(half, weights_ref, first_ref, second_ref, *refs):
    backs = refs[:EXPERTS]
    token_ref, route_ref = refs[EXPERTS:]
    back = jnp.concatenate([b[...] for b in backs], axis=0)
    first, second = first_ref[...], second_ref[...]
    token_ref[...] = dot_f32(first + second, back[:, :half], 1, 0).astype(BF)
    share = back[:, half:]
    route_ref[0:1] = dot_f32(share, first, 0, 1)[0:1] / weights_ref[0:1]
    route_ref[1:2] = dot_f32(share, second, 0, 1)[0:1] / weights_ref[1:2]


def combine(weights, first, second, backs):
    rows = weights.shape[1]
    half = backs[0].shape[1] - LANES
    return pl.pallas_call(
        functools.partial(final_kernel, half),
        out_shape=[
            jax.ShapeDtypeStruct((rows, half), BF),
            jax.ShapeDtypeStruct((TOP, rows), F32),
        ],
        in_specs=[VMEM] * (3 + EXPERTS),
        out_specs=[VMEM] * 2,
        compiler_params=pltpu.CompilerParams(vmem_limit_bytes=8 * MIB),
        cost_estimate=pl.CostEstimate(
            flops=2 * 128 * 24 * half, bytes_accessed=MIB, transcendentals=0
        ),
        name="combine",
    )(weights, first, second, *backs)


def per_device(tokens, cotangent, routes, route_weights, gate_weight, up_weight, down_weight):
    place = jnp.stack([lax.axis_index("core"), lax.axis_index("z"), lax.axis_index("yh")])
    place = place.astype(jnp.int32)
    packed = EXPERTS * CAP
    third = packed // 3

    made = make_slots(place, tokens, cotangent, routes.T, route_weights.T)
    first, second = made[EXPERTS:]
    part = packed // 2
    row_of = jnp.arange(part)
    pack = (
        (row_of // CAP * ROOM + row_of % CAP)[:, None] == jnp.arange(EXPERTS * ROOM // 2)[None, :]
    ).astype(BF)

    def packing(sent, dy):
        got = list(sent)
        for dz in (2, 1, 3, 0):
            if dz or dy:
                got[dz] = to_expert(sent[dz], dz, dy, 1)
        return dot_f32(pack, jnp.concatenate(got, axis=0), 1, 0).astype(BF)

    own, left, right, partner, far_left, far_right, across = ([] for _ in range(7))
    own = [packing(made[h:EXPERTS:2], h) for h in range(2)]
    for h in range(2):
        left.append(along_x(own[h], 1))
        right.append(along_x(own[h], -1))
        partner.append(pair_y(own[h]))
    for h in range(2):
        far_left.append(along_x(partner[h], 1))
        far_right.append(pair_y(right[h]))
        across.append(along_x(right[h], -1))

    down_t = down_weight[0]
    hid = down_t.shape[0]
    pair_t = stack_weights(gate_weight[0].T, up_weight[0].T)
    near = own + left + right + partner
    near_other = [pair_core(v) for v in near]
    near_out = run_group(place, near, near_other, pair_t, down_t)
    tied = lax.optimization_barrier((far_left[0], far_right[0], *near_out))
    far_left[0], far_right[0] = tied[:2]
    near_out = tied[2:]
    early = [along_x(far_left[0][:third], 1), along_x(far_right[0][third:], -1)]
    far = far_left + far_right + across
    rest = packed - 2 * third - third // 2
    last = early + [along_x(far_left[1][:rest], 1), pair_y(across[1][rest:])]
    far = far + last
    far_other = [pair_core(v) for v in far]
    far_out = run_group(place, far, far_other, pair_t, down_t)

    def add(a, *more):
        total = a.astype(F32)
        for m in more:
            total = total + m.astype(F32)
        return total.astype(BF)

    far_got = pair_core(far_out[0])
    near_got = pair_core(near_out[0])
    far_keep = keep_half(place, far_out[2], far_out[1], pair_t)
    near_keep = keep_half(place, near_out[2], near_out[1], pair_t)

    def chunk(keep, got, i, a=0, b=packed):
        return add(keep[packed * i + a : packed * i + b], got[packed * i + a : packed * i + b])

    t_last = [chunk(far_keep, far_got, 3, third * i, third * (i + 1)) for i in range(3)]
    a_left = along_x(t_last[0], -1)
    a_right = along_x(t_last[1], 1)
    a_pair = pair_y(t_last[2])
    pads = [[(third * i, packed - third * (i + 1)), (0, 0)] for i in range(3)]
    t_far_left = add(chunk(far_keep, far_got, 0), jnp.pad(a_left, pads[0]))
    t_far_right = add(chunk(far_keep, far_got, 1), jnp.pad(a_right, pads[1]))
    t_across = add(chunk(far_keep, far_got, 2), jnp.pad(a_pair, pads[2]))
    b_partner = along_x(t_far_left, -1)
    b_right_pair = pair_y(t_far_right)
    b_right = along_x(t_across, 1)
    rows = (near + far, near_other + far_other)
    sides = [near_out[2], far_out[2]]
    gate_grad, up_grad = weight_grads(place, *rows, sides, 0, hid)
    tied = lax.optimization_barrier((b_partner, b_right_pair, b_right, gate_grad, up_grad))
    b_partner, b_right_pair, b_right, gate_grad, up_grad = tied
    c_left = along_x(chunk(near_keep, near_got, 1), -1)
    c_right = along_x(add(chunk(near_keep, near_got, 2), b_right_pair, b_right), 1)
    c_pair = pair_y(add(chunk(near_keep, near_got, 3), b_partner))
    half = tokens.shape[1] // 2
    (down_grad,) = weight_grads(place, *rows, [near_out[3], far_out[3]], half, hid)
    tied = lax.optimization_barrier((c_left, c_right, c_pair, down_grad))
    c_left, c_right, c_pair, down_grad = tied
    home = add(chunk(near_keep, near_got, 0), c_left, c_right, c_pair)

    backs = [None] * EXPERTS
    for dy in range(2):
        spread = dot_f32(pack, home[part * dy : part * (dy + 1)], 0, 0).astype(BF)
        for dz in (2, 1, 3, 0):
            k = 2 * dz + dy
            piece = spread[ROOM * dz : ROOM * (dz + 1)]
            if k:
                piece = to_expert(piece, dz, dy, -1)
            backs[k] = piece
    token_grad, route_grad = combine(route_weights.T, first, second, backs)

    return token_grad, route_grad.T, gate_grad.T[None], up_grad.T[None], down_grad[None]


def solution(mesh):
    names = ("z", "yh", "yl", "x", "core")
    fine = Mesh(mesh.devices.reshape(4, 2, 2, 4, 2), names)
    ep = names[:4]
    return jax.shard_map(
        per_device,
        mesh=fine,
        in_specs=(
            P(ep, None),
            P(ep, None),
            P(ep, None),
            P(ep, None),
            P(ep, None, "core"),
            P(ep, None, "core"),
            P(ep, "core", None),
        ),
        out_specs=(
            P(ep, "core"),
            P(ep, None),
            P(ep, None, "core"),
            P(ep, None, "core"),
            P(ep, "core", None),
        ),
        check_vma=False,
    )
```

```python
import functools

import jax
import jax.numpy as jnp
from jax import lax
from jax.experimental import pallas as pl
from jax.experimental.pallas import tpu as pltpu
from jax.sharding import Mesh
from jax.sharding import PartitionSpec as P


EXPERTS = 8
TOP = 2
CAP = 12
ROOM = 16
LANES = 128
BF = jnp.bfloat16
F32 = jnp.float32
MIB = 1 << 20


VMEM = pl.BlockSpec(memory_space=pltpu.VMEM)
SMEM = pl.BlockSpec(memory_space=pltpu.SMEM)


def along_x(value, step):
    return lax.ppermute(value, "x", [(i, (i + step) % 4) for i in range(4)])


def pair_y(value):
    return lax.ppermute(value, "yl", [(0, 1), (1, 0)])


def pair_core(value):
    return lax.ppermute(value, "core", [(0, 1), (1, 0)])


def to_expert(value, dz, dy, sign):
    perm = []
    for z in range(4):
        for y in range(4):
            there = (z + sign * dz) % 4 * 4 + (3 - y if dy else y)
            perm.append((z * 4 + y, there))
    return lax.ppermute(value, ("z", "yh", "yl"), perm)


def dot_f32(a, b, left, right):
    return lax.dot_general(a, b, (((left,), (right,)), ((), ())), preferred_element_type=F32)


def slots_kernel(half, place_ref, tok_ref, cot_ref, routes_ref, weights_ref, *refs):
    core, z, yh = place_ref[0], place_ref[1], place_ref[2]
    outs = refs[:EXPERTS]
    first_ref, second_ref, tok_half, cot_half, sems = refs[EXPERTS:]
    here = pl.ds(pl.multiple_of(core * half, half), half)
    loads = [
        pltpu.make_async_copy(tok_ref.at[:, here], tok_half, sems.at[0]),
        pltpu.make_async_copy(cot_ref.at[:, here], cot_half, sems.at[1]),
    ]
    for c in loads:
        c.start()
    rows = tok_half.shape[0]
    routes = routes_ref[...].T
    weights = weights_ref[...].T
    slot = lax.broadcasted_iota(jnp.int32, (rows, EXPERTS * ROOM), 1)
    index = slot // ROOM
    expert = 2 * ((z + index // 2) % 4) + (yh + index % 2) % 2
    is_first = routes[:, 0:1] == expert
    is_second = routes[:, 1:2] == expert
    hot = jnp.where(is_first | is_second, 1.0, 0.0).astype(BF)
    below = lax.broadcasted_iota(jnp.int32, (rows, rows), 1) < lax.broadcasted_iota(
        jnp.int32, (rows, rows), 0
    )
    position = dot_f32(jnp.where(below, 1.0, 0.0).astype(BF), hot, 1, 0)
    fits = position == (slot % ROOM).astype(F32)
    first = jnp.where(is_first & fits, 1.0, 0.0).astype(BF)
    second = jnp.where(is_second & fits, 1.0, 0.0).astype(BF)
    first_ref[...] = first
    second_ref[...] = second
    for c in loads:
        c.wait()
    slot_tok = dot_f32(first + second, tok_half[...], 0, 0).astype(BF)
    cot = cot_half[...].astype(F32)
    scaled = dot_f32(first, (cot * weights[:, 0:1]).astype(BF), 0, 0)
    scaled = scaled + dot_f32(second, (cot * weights[:, 1:2]).astype(BF), 0, 0)
    scaled = scaled.astype(BF)
    for k in range(EXPERTS):
        outs[k][:, :half] = slot_tok[k * ROOM : (k + 1) * ROOM]
        outs[k][:, half:] = scaled[k * ROOM : (k + 1) * ROOM]


def make_slots(place, tokens, cotangent, routes, weights):
    rows, width = tokens.shape
    shapes = [jax.ShapeDtypeStruct((ROOM, width), BF)] * EXPERTS
    shapes += [jax.ShapeDtypeStruct((rows, EXPERTS * ROOM), BF)] * 2
    anywhere = pl.BlockSpec(memory_space=pl.ANY)
    return pl.pallas_call(
        functools.partial(slots_kernel, width // 2),
        out_shape=shapes,
        in_specs=[SMEM, anywhere, anywhere, VMEM, VMEM],
        out_specs=[VMEM] * len(shapes),
        scratch_shapes=[
            pltpu.VMEM((rows, width // 2), BF),
            pltpu.VMEM((rows, width // 2), BF),
            pltpu.SemaphoreType.DMA((2,)),
        ],
        compiler_params=pltpu.CompilerParams(vmem_limit_bytes=60 * MIB),
        cost_estimate=pl.CostEstimate(
            flops=2 * 128 * 24 * width * 2, bytes_accessed=3 * MIB, transcendentals=0
        ),
        name="slots",
    )(place, tokens, cotangent, routes, weights)


def stack_kernel(gate_ref, up_ref, out_ref):
    hid = gate_ref.shape[0]
    wide = out_ref.shape[0] // 2
    for i, ref in enumerate((gate_ref, up_ref)):
        out_ref[wide * i : wide * i + hid] = ref[...]
        out_ref[wide * i + hid : wide * (i + 1)] = jnp.zeros((wide - hid, ref.shape[1]), BF)


def stack_weights(gate, up):
    hid, width = gate.shape
    return pl.pallas_call(
        stack_kernel,
        out_shape=jax.ShapeDtypeStruct((2 * padded(hid), width), BF),
        in_specs=[VMEM] * 2,
        out_specs=VMEM,
        compiler_params=pltpu.CompilerParams(vmem_limit_bytes=16 * MIB),
        cost_estimate=pl.CostEstimate(flops=1000, bytes_accessed=12 * MIB, transcendentals=0),
        name="stack",
    )(gate, up)


def padded(n):
    return -(-n // LANES) * LANES


def group_kernel(count, half, place_ref, *refs):
    core = place_ref[0]
    ours, theirs = refs[:count], refs[count : 2 * count]
    pair_ref, down_ref = refs[2 * count : 2 * count + 2]
    send_ref, share_out, sides_out, hidden_out = refs[2 * count + 2 :]
    hid = down_ref.shape[0]
    wide = hidden_out.shape[1]
    here = pl.ds(pl.multiple_of(core * half, half), half)
    there = pl.ds(pl.multiple_of((1 - core) * half, half), half)
    tok = [jnp.concatenate([r[:, :half] for r in side], axis=0) for side in (ours, theirs)]
    pair = dot_f32(tok[0], pair_ref[:, here], 1, 1) + dot_f32(tok[1], pair_ref[:, there], 1, 1)
    cot = [jnp.concatenate([r[:, half:] for r in side], axis=0) for side in (ours, theirs)]
    grad = dot_f32(cot[0], down_ref[:, here], 1, 1) + dot_f32(cot[1], down_ref[:, there], 1, 1)
    gate, up = pair[:, :hid], pair[:, wide : wide + hid]
    sigma = 1.0 / (1.0 + jnp.exp(-gate))
    active = gate * sigma
    hidden = (active * up).astype(BF)
    gate_side = (grad * up * (sigma * (1.0 + gate * (1.0 - sigma)))).astype(BF)
    up_side = (grad * active).astype(BF)
    rest = jnp.zeros((hidden.shape[0], wide - hid), BF)
    hidden_out[:, :hid] = hidden
    hidden_out[:, hid:] = rest
    sides_out[:, :hid] = gate_side
    sides_out[:, hid:wide] = rest
    sides_out[:, wide : wide + hid] = up_side
    sides_out[:, wide + hid :] = rest
    share = jnp.sum(hidden.astype(F32) * grad, axis=1, keepdims=True).astype(BF)
    share = jnp.broadcast_to(share, (share.shape[0], LANES))
    share_out[...] = share
    token_terms(sides_out, pair_ref, share, (1 - core) * half, send_ref)


def token_terms(sides_ref, pair_ref, share, base, out):
    half = out.shape[1] - LANES
    tile = 1024
    out[:, half:] = share

    @pl.loop(0, half // tile)
    def _(j):
        where = pl.ds(pl.multiple_of(base + j * tile, tile), tile)
        term = dot_f32(sides_ref[...], pair_ref[:, where], 1, 0)
        out[:, pl.ds(pl.multiple_of(j * tile, tile), tile)] = term.astype(BF)


def keep_kernel(half, place_ref, sides_ref, share_ref, pair_ref, out_ref):
    token_terms(sides_ref, pair_ref, share_ref[...], place_ref[0] * half, out_ref)


def keep_half(place, sides, share, pair):
    rows = sides.shape[0]
    half = pair.shape[1] // 2
    return pl.pallas_call(
        functools.partial(keep_kernel, half),
        out_shape=jax.ShapeDtypeStruct((rows, half + LANES), BF),
        in_specs=[SMEM] + [VMEM] * 3,
        out_specs=VMEM,
        compiler_params=pltpu.CompilerParams(vmem_limit_bytes=12 * MIB),
        cost_estimate=pl.CostEstimate(
            flops=2 * rows * pair.shape[0] * half, bytes_accessed=8 * MIB, transcendentals=0
        ),
        name="keep",
    )(place, sides, share, pair)


def run_group(place, ours, theirs, pair, down):
    rows = sum(r.shape[0] for r in ours)
    hid, width = down.shape
    half = width // 2
    lanes = (half + LANES, LANES, 2 * padded(hid), padded(hid))
    shapes = [jax.ShapeDtypeStruct((rows, n), BF) for n in lanes]
    return pl.pallas_call(
        functools.partial(group_kernel, len(ours), half),
        out_shape=shapes,
        in_specs=[SMEM] + [VMEM] * (2 * len(ours) + 2),
        out_specs=[VMEM] * len(shapes),
        compiler_params=pltpu.CompilerParams(vmem_limit_bytes=20 * MIB),
        cost_estimate=pl.CostEstimate(
            flops=8 * rows * hid * width, bytes_accessed=16 * MIB, transcendentals=rows * hid
        ),
        name="group",
    )(place, *ours, *theirs, pair, down)


def weight_kernel(sizes, offset, half, hid, tile, place_ref, *refs):
    count = len(sizes)
    kinds = len(refs) - 2 * count - 5
    ours, theirs = refs[:count], refs[count : 2 * count]
    sides = refs[2 * count : 2 * count + 2]
    outs = refs[2 * count + 2 : 2 * count + 2 + kinds]
    sides_t, stage, out_sem = refs[2 * count + 2 + kinds :]
    core = place_ref[0]
    depth = sides[0].shape[0]
    wide = sides[0].shape[1] // kinds
    for i in range(2):
        sides_t[:, depth * i : depth * (i + 1)] = sides[i][...].T
    stores = []
    for s, group in enumerate((ours, theirs)):
        base = (core if s == 0 else 1 - core) * half

        @pl.loop(0, half // tile)
        def _(j):
            to = pl.ds(pl.multiple_of(base + j * tile, tile), tile)
            lanes = pl.ds(pl.multiple_of(offset + j * tile, tile), tile)
            block = jnp.concatenate([r[:, lanes] for r in group], axis=0)
            grads = dot_f32(sides_t[...], block, 1, 0).astype(BF)
            for k in range(kinds):
                stage[k, :, to] = grads[wide * k : wide * k + hid]

        whole = pl.ds(pl.multiple_of(base, half), half)
        for k in range(kinds):
            copy = pltpu.make_async_copy(
                stage.at[k, :, whole], outs[k].at[:, whole], out_sem.at[s, k]
            )
            copy.start()
            stores.append(copy)
    for copy in stores:
        copy.wait()


def weight_grads(place, ours, theirs, sides, offset, hid, tile=1024):
    sizes = [r.shape[0] for r in ours]
    rows = sum(sizes)
    width = ours[0].shape[1]
    wide = padded(hid)
    kinds = sides[0].shape[1] // wide
    anywhere = pl.BlockSpec(memory_space=pl.ANY)
    return pl.pallas_call(
        functools.partial(weight_kernel, sizes, offset, width // 2, hid, tile),
        out_shape=[jax.ShapeDtypeStruct((hid, width), BF)] * kinds,
        in_specs=[SMEM] + [VMEM] * (2 * len(sizes) + len(sides)),
        out_specs=[anywhere] * kinds,
        scratch_shapes=[
            pltpu.VMEM((kinds * wide, rows), BF),
            pltpu.VMEM((kinds, hid, width), BF),
            pltpu.SemaphoreType.DMA((2, kinds)),
        ],
        compiler_params=pltpu.CompilerParams(vmem_limit_bytes=18 * MIB),
        cost_estimate=pl.CostEstimate(
            flops=2 * kinds * rows * hid * width, bytes_accessed=14 * MIB, transcendentals=0
        ),
        name="weight_grads",
    )(place, *ours, *theirs, *sides)


def final_kernel(half, weights_ref, first_ref, second_ref, *refs):
    backs = refs[:EXPERTS]
    token_ref, route_ref = refs[EXPERTS:]
    back = jnp.concatenate([b[...] for b in backs], axis=0)
    first, second = first_ref[...], second_ref[...]
    token_ref[...] = dot_f32(first + second, back[:, :half], 1, 0).astype(BF)
    share = back[:, half:]
    route_ref[0:1] = dot_f32(share, first, 0, 1)[0:1] / weights_ref[0:1]
    route_ref[1:2] = dot_f32(share, second, 0, 1)[0:1] / weights_ref[1:2]


def combine(weights, first, second, backs):
    rows = weights.shape[1]
    half = backs[0].shape[1] - LANES
    return pl.pallas_call(
        functools.partial(final_kernel, half),
        out_shape=[
            jax.ShapeDtypeStruct((rows, half), BF),
            jax.ShapeDtypeStruct((TOP, rows), F32),
        ],
        in_specs=[VMEM] * (3 + EXPERTS),
        out_specs=[VMEM] * 2,
        compiler_params=pltpu.CompilerParams(vmem_limit_bytes=8 * MIB),
        cost_estimate=pl.CostEstimate(
            flops=2 * 128 * 24 * half, bytes_accessed=MIB, transcendentals=0
        ),
        name="combine",
    )(weights, first, second, *backs)


def per_device(tokens, cotangent, routes, route_weights, gate_weight, up_weight, down_weight):
    place = jnp.stack([lax.axis_index("core"), lax.axis_index("z"), lax.axis_index("yh")])
    place = place.astype(jnp.int32)
    packed = EXPERTS * CAP
    third = packed // 3

    made = make_slots(place, tokens, cotangent, routes.T, route_weights.T)
    first, second = made[EXPERTS:]
    part = packed // 2
    row_of = jnp.arange(part)
    pack = (
        (row_of // CAP * ROOM + row_of % CAP)[:, None] == jnp.arange(EXPERTS * ROOM // 2)[None, :]
    ).astype(BF)

    def packing(sent, dy):
        got = list(sent)
        for dz in (2, 1, 3, 0):
            if dz or dy:
                got[dz] = to_expert(sent[dz], dz, dy, 1)
        return dot_f32(pack, jnp.concatenate(got, axis=0), 1, 0).astype(BF)

    own, left, right, partner, far_left, far_right, across = ([] for _ in range(7))
    own = [packing(made[h:EXPERTS:2], h) for h in range(2)]
    for h in range(2):
        left.append(along_x(own[h], 1))
        right.append(along_x(own[h], -1))
        partner.append(pair_y(own[h]))
    for h in range(2):
        far_left.append(along_x(partner[h], 1))
        far_right.append(pair_y(right[h]))
        across.append(along_x(right[h], -1))

    down_t = down_weight[0]
    hid = down_t.shape[0]
    pair_t = stack_weights(gate_weight[0].T, up_weight[0].T)
    near = own + left + right + partner
    near_other = [pair_core(v) for v in near]
    near_out = run_group(place, near, near_other, pair_t, down_t)
    tied = lax.optimization_barrier((far_left[0], far_right[0], *near_out))
    far_left[0], far_right[0] = tied[:2]
    near_out = tied[2:]
    early = [along_x(far_left[0][:third], 1), along_x(far_right[0][third:], -1)]
    far = far_left + far_right + across
    rest = packed - 2 * third - third // 2
    last = early + [along_x(far_left[1][:rest], 1), pair_y(across[1][rest:])]
    far = far + last
    far_other = [pair_core(v) for v in far]
    far_out = run_group(place, far, far_other, pair_t, down_t)

    def add(a, *more):
        total = a.astype(F32)
        for m in more:
            total = total + m.astype(F32)
        return total.astype(BF)

    far_got = pair_core(far_out[0])
    near_got = pair_core(near_out[0])
    far_keep = keep_half(place, far_out[2], far_out[1], pair_t)
    near_keep = keep_half(place, near_out[2], near_out[1], pair_t)

    def chunk(keep, got, i, a=0, b=packed):
        return add(keep[packed * i + a : packed * i + b], got[packed * i + a : packed * i + b])

    c_left = along_x(chunk(near_keep, near_got, 1), -1)
    t_last = [chunk(far_keep, far_got, 3, third * i, third * (i + 1)) for i in range(3)]
    a_left = along_x(t_last[0], -1)
    a_right = along_x(t_last[1], 1)
    a_pair = pair_y(t_last[2])
    pads = [[(third * i, packed - third * (i + 1)), (0, 0)] for i in range(3)]
    t_far_left = add(chunk(far_keep, far_got, 0), jnp.pad(a_left, pads[0]))
    t_far_right = add(chunk(far_keep, far_got, 1), jnp.pad(a_right, pads[1]))
    t_across = add(chunk(far_keep, far_got, 2), jnp.pad(a_pair, pads[2]))
    b_right_pair = pair_y(t_far_right)
    b_right = along_x(t_across, 1)
    b_partner = along_x(t_far_left, -1)
    rows = (near + far, near_other + far_other)
    sides = [near_out[2], far_out[2]]
    gate_grad, up_grad = weight_grads(place, *rows, sides, 0, hid)
    tied = lax.optimization_barrier((b_partner, b_right_pair, b_right, gate_grad, up_grad))
    b_partner, b_right_pair, b_right, gate_grad, up_grad = tied
    half = tokens.shape[1] // 2
    (down_grad,) = weight_grads(place, *rows, [near_out[3], far_out[3]], half, hid)
    c_right, c_pair = [], []
    for h in range(2):
        span = (part * h, part * (h + 1))
        cut = slice(*span)
        value = add(chunk(near_keep, near_got, 2, *span), b_right_pair[cut], b_right[cut])
        c_right.append(along_x(value, 1))
        value = add(chunk(near_keep, near_got, 3, *span), b_partner[cut])
        c_pair.append(pair_y(value))
    backs = [None] * EXPERTS
    base = (near_keep, near_got, c_left)
    for h in range(2):
        span = (part * h, part * (h + 1))
        home = add(chunk(base[0], base[1], 0, *span), base[2][slice(*span)], c_right[h], c_pair[h])
        if h == 0:
            home, *base = lax.optimization_barrier((home, *base))
        spread = dot_f32(pack, home, 0, 0).astype(BF)
        for dz in (2, 1, 3, 0):
            piece = spread[ROOM * dz : ROOM * (dz + 1)]
            if dz or h:
                piece = to_expert(piece, dz, h, -1)
            backs[2 * dz + h] = piece
    token_grad, route_grad = combine(route_weights.T, first, second, backs)

    return token_grad, route_grad.T, gate_grad.T[None], up_grad.T[None], down_grad[None]


def solution(mesh):
    names = ("z", "yh", "yl", "x", "core")
    fine = Mesh(mesh.devices.reshape(4, 2, 2, 4, 2), names)
    ep = names[:4]
    return jax.shard_map(
        per_device,
        mesh=fine,
        in_specs=(
            P(ep, None),
            P(ep, None),
            P(ep, None),
            P(ep, None),
            P(ep, None, "core"),
            P(ep, None, "core"),
            P(ep, "core", None),
        ),
        out_specs=(
            P(ep, "core"),
            P(ep, None),
            P(ep, None, "core"),
            P(ep, None, "core"),
            P(ep, "core", None),
        ),
        check_vma=False,
    )
```
